256 devices in a mesh: ep: 64 (over z, x, core), tp: 4 (over y).
Axes of the slice: x: 4, y: 4, z: 8, core: 2. Of those that a mesh axis runs over, the one named last changes fastest.
Arguments:
- mixer_input: bfloat16 [32768, 2048], P('ep'), may hold values from -5.5 to 5.5
- expert_input: bfloat16 [32768, 2048], P('ep'), may hold values from -6 to 6
- gain_mixer: float32 [2048], replicated, may hold values from 0.1 to 1.9
- gain_expert: float32 [2048], replicated, may hold values from 0.1 to 1.9
- query_weight: bfloat16 [2048, 1536], P(None, 'tp')
- key_weight: bfloat16 [2048, 256], P(None, 'tp')
- value_weight: bfloat16 [2048, 256], P(None, 'tp'), may hold values from -0.125 to 0.125
- sink_logits: float32 [24], P('tp'), may hold values from 2 to 6
- output_weight: bfloat16 [1536, 2048], P('tp'), may hold values from -0.75 to 0.75
- expert_choice: int32 [32768, 2], P('ep'), may hold values from 0 to 63, all different within a row; in each aligned block of 128 rows (0 to 127, 128 to 255, ...) at most 8 rows name the same one
- route_weights: float32 [32768, 2], P('ep'), may hold values from 0.2 to 1.2
- expert_gate: bfloat16 [64, 2048, 1024], P('ep', None, 'tp'), may hold values from -0.125 to 0.125
- expert_up: bfloat16 [64, 2048, 1024], P('ep', None, 'tp'), may hold values from -0.125 to 0.125
- expert_down: bfloat16 [64, 1024, 2048], P('ep', 'tp'), may hold values from -0.1875 to 0.1875
- shared_gate: bfloat16 [2048, 512], P(None, 'tp'), may hold values from -0.125 to 0.125
- shared_up: bfloat16 [2048, 512], P(None, 'tp'), may hold values from -0.125 to 0.125
- shared_down: bfloat16 [512, 2048], P('tp'), may hold values from -0.25 to 0.25
Outputs:
- mixer_output: bfloat16 [32768, 2048], P(('ep', 'tp'))
- expert_output: bfloat16 [32768, 2048], P(('ep', 'tp'))
The draws below stay inside these ranges and needn't reach their ends.
Inputs may be any that keep to these rules, and one draw needn't show every extreme that they name: `expert_choice`: in each aligned block of 128 rows no expert is named by more than 8 rows, and in some block some expert is named by exactly 8 rows; the 2 entries of a row differ.
All inputs are finite; a program needn't handle non-finite values.
Results may differ from the reference program's by a relative error of at most 0.019.
Values may be sent and summed in bfloat16 or wider, within the bound.
No kernel may reach another device: no remote copies, remote signals or barrier semaphores. Data moves between devices by JAX's collectives and lax.ppermute only.
A program may use at most 128 MiB of HBM per device.

```python
import math
import jax
import jax.numpy as jnp
import numpy as np
from jax import lax

D = 2048
HEADS = 24
KV_HEADS = 4
HEAD_DIM = 64
WINDOW = 128
SEQS = 1
EXPERT_FF = 1024
SHARED_FF = 512
TOP = 2
TOK_B_DEV = 128
EXPERTS = 64
TOKENS_A = 32768
TOKENS_B = 32768
SEQ_LEN = 32768
CAP = 8
N_TP = 4


def attention_weights(key):
    base_key = jax.random.fold_in(key, 41)
    key_part = jax.random.truncated_normal(jax.random.fold_in(base_key, 1), -4.0, 4.0, (D, KV_HEADS * HEAD_DIM), jnp.float32) * D ** (-0.5)
    query_part = jax.random.truncated_normal(jax.random.fold_in(base_key, 2), -4.0, 4.0, (D, HEADS * HEAD_DIM), jnp.float32) * D ** (-0.5)
    return (key_part, query_part)


def draw_key_weight(key, part):
    key_part, query_part = attention_weights(key)
    return key_part.astype(jnp.bfloat16)


def draw_query_weight(key, part):
    key_part, query_part = attention_weights(key)
    return query_part.astype(jnp.bfloat16)


def draw_mixer_input(key, part):
    base_key = jax.random.fold_in(key, 53)
    values = jax.random.truncated_normal(jax.random.fold_in(base_key, 1), -5.0, 5.0, (TOKENS_A, D), jnp.float32)
    return values.astype(jnp.bfloat16)


def steps_of(stream_key, dims, pieces, low, largest):
    def one(axis_at, parts):
        draws = jax.random.uniform(jax.random.fold_in(jax.random.fold_in(stream_key, 6), axis_at), (parts,), jnp.float32, low / len(pieces), largest / len(pieces))
        return jnp.repeat(jnp.exp(draws), dims[axis_at] // parts).reshape((-1,) + (1,) * (len(dims) - axis_at - 1))

    loudness = one(*pieces[0])
    for cut in pieces[1:]:
        loudness = loudness * one(*cut)
    return loudness


def deal_out(stream_key, own, number, rows, amount, top, most, lean):
    ranking = jax.random.permutation(stream_key, amount)
    crowded, ordinary = shares(amount, rows * top, most, lean, True), shares(amount, rows * top, most, lean, False)
    places = jnp.arange(amount)

    def named(tallies, turn):
        used = int((tallies > 0).sum())
        fixed = max(1, used // 4)
        moved = fixed + (places - fixed + turn * (used - fixed)) % max(1, amount - fixed)
        return jnp.zeros((amount,), jnp.int32).at[ranking[jnp.where(places < fixed, places, moved)]].set(jnp.asarray(tallies, jnp.int32))

    tallies = jnp.where(number % 4 == 0, named(crowded, number // 4), named(ordinary, number - number // 4 - 1))
    mixed = jax.random.permutation(jax.random.fold_in(own, 3), amount)
    source_of, sink = mixed[0:amount // 2 * 2:2], mixed[1:amount // 2 * 2:2]
    margin = jnp.minimum(tallies[source_of] - 1, most - tallies[sink]) // 2
    margin = jnp.where((source_of == ranking[0]) | (sink == ranking[0]) | (tallies[sink] == 0), 0, jnp.maximum(margin, 0))
    moved = jax.random.randint(jax.random.fold_in(own, 4), (amount // 2,), 0, 1 << 20) % (margin + 1)
    tallies = tallies.at[source_of].add(-moved).at[sink].add(moved)
    items = jnp.searchsorted(jnp.cumsum(tallies), jnp.arange(rows * top), side="right").astype(jnp.int32)
    listing = items.reshape(top, rows).T
    listing = listing[jax.random.permutation(jax.random.fold_in(own, 1), rows)]
    turn = jax.random.randint(jax.random.fold_in(own, 2), (rows, 1), 0, top)
    return jnp.take_along_axis(listing, (jnp.arange(top)[None, :] + turn) % top, axis=1)


def shares(number_of, total, bound, skew, full):
    loads = [(1 << 20) // math.isqrt(grade ** skew) + 1 for grade in range(1, number_of + 1)]
    largest = bound if full else min(bound, max(-(-total // number_of), total * loads[0] // sum(loads)))
    least = 1 if total - largest >= number_of - 1 else 0
    counts, surplus = [largest] + [least] * (number_of - 1), total - largest - least * (number_of - 1)
    while surplus > 0:
        movable = [i for i in range(1, number_of) if counts[i] < largest] or [i for i in range(1, number_of) if counts[i] < bound]
        whole, remaining = sum([loads[i] for i in movable]), surplus
        for i in movable:
            more = min(bound - counts[i], max(1, remaining * loads[i] // whole), surplus)
            counts[i] = counts[i] + more
            surplus = surplus - more
    return np.array(counts)


def bell_draw(own_key, dims, scale, bound, pieces=(), kind=jnp.bfloat16):
    entries = jax.random.normal(own_key, dims, jnp.float32) * scale
    if len(pieces) > 0:
        entries = steps_of(own_key, dims, pieces, -0.22, 0.18) * entries
    return jnp.clip(entries, min=-bound, max=bound).astype(kind)


def setup_inputs(seed: int = 0) -> dict:
    key_of = jax.random.split(jax.random.key(seed), 18)
    mixer_input = draw_mixer_input(jax.random.fold_in(key_of[17], 71), 0)
    expert_input = bell_draw(key_of[1], (TOKENS_B, D), 1.0, 6.0, ((0, 64),))
    gain_mixer = jnp.clip(1.0 + 0.18 * jax.random.normal(key_of[2], (D,), jnp.float32), 0.1, 1.9)
    gain_expert = jnp.clip(1.0 + 0.18 * jax.random.normal(key_of[3], (D,), jnp.float32), 0.1, 1.9)
    query_weight = draw_query_weight(jax.random.fold_in(key_of[17], 71), 0)
    key_weight = draw_key_weight(jax.random.fold_in(key_of[17], 71), 0)
    value_weight = bell_draw(key_of[6], (D, KV_HEADS * HEAD_DIM), D ** -0.5, 0.125, ((1, 4),))
    sink_logits = jnp.clip(2.0 + 4.0 * jax.random.uniform(key_of[7], (HEADS,), jnp.float32) ** steps_of(key_of[7], (HEADS,), ((0, 4),), -0.2, 0.2), 2.0, 6.0)
    output_weight = bell_draw(key_of[8], (HEADS * HEAD_DIM, D), (HEADS * HEAD_DIM // 25) ** -0.5, 0.75, ((0, 4),))
    expert_choice_keys = jax.random.split(jax.random.fold_in(key_of[9], 1), TOKENS_B // TOK_B_DEV)
    expert_choice_turns = jax.random.permutation(jax.random.fold_in(key_of[9], 3), TOKENS_B // TOK_B_DEV)
    expert_choice = jax.vmap(lambda own, number: deal_out(jax.random.fold_in(key_of[9], 2), own, number, TOK_B_DEV, EXPERTS, TOP, CAP, 2))(expert_choice_keys, expert_choice_turns).reshape((TOKENS_B, TOP))
    route_weights = jnp.clip(0.2 + 1 * jax.random.uniform(key_of[10], (TOKENS_B, TOP), jnp.float32) ** steps_of(key_of[10], (TOKENS_B, TOP), ((0, 64),), -0.2, 0.2), 0.2, 1.2)
    expert_gate = bell_draw(key_of[11], (EXPERTS, D, EXPERT_FF), D ** -0.5, 0.125, ((0, 64), (2, 4)))
    expert_up = bell_draw(key_of[12], (EXPERTS, D, EXPERT_FF), D ** -0.5, 0.125, ((0, 64), (2, 4)))
    expert_down = bell_draw(key_of[13], (EXPERTS, EXPERT_FF, D), EXPERT_FF ** -0.5, 0.1875, ((0, 64), (1, 4)))
    shared_gate = bell_draw(key_of[14], (D, SHARED_FF), D ** -0.5, 0.125, ((1, 4),))
    shared_up = bell_draw(key_of[15], (D, SHARED_FF), D ** -0.5, 0.125, ((1, 4),))
    shared_down = bell_draw(key_of[16], (SHARED_FF, D), SHARED_FF ** -0.5, 0.25, ((0, 4),))
    return dict(mixer_input=mixer_input, expert_input=expert_input, gain_mixer=gain_mixer, gain_expert=gain_expert, query_weight=query_weight, key_weight=key_weight, value_weight=value_weight, sink_logits=sink_logits, output_weight=output_weight, expert_choice=expert_choice, route_weights=route_weights, expert_gate=expert_gate, expert_up=expert_up, expert_down=expert_down, shared_gate=shared_gate, shared_up=shared_up, shared_down=shared_down)


norm_eps = 1e-06
rope_base = 500000.0

def rounded(value):
    return lax.optimization_barrier(value.astype(jnp.bfloat16)).astype(jnp.float32)

def rms_scale(matrix, scaling):
    widened = matrix.astype(jnp.float32)
    scaled = widened * lax.rsqrt(lax.optimization_barrier(jnp.mean(widened * widened, axis=-1, keepdims=True)) + norm_eps)
    return (scaled * scaling).astype(jnp.bfloat16)

def frequencies(head_size):
    half_steps = jnp.arange(head_size // 2, dtype=jnp.float32)
    return rope_base ** (-(2.0 * half_steps) / head_size)

def rotate(heads, angles):
    middle = heads.shape[-1] // 2
    widened = heads.astype(jnp.float32)
    cosine = jnp.cos(angles)[:, None, :]
    sine_val = jnp.sin(angles)[:, None, :]
    leading = widened[..., :middle]
    trailing = widened[..., middle:]
    turned = jnp.concatenate([leading * cosine - trailing * sine_val, trailing * cosine + leading * sine_val], axis=-1)
    return turned.astype(jnp.bfloat16)

def attend(query_heads, key_heads, value_heads, prior_keys, prior_values, first_position, sink_logits):
    window = prior_keys.shape[0]
    total_rows, kv_count, head_size = key_heads.shape
    group_size = query_heads.shape[1] // kv_count
    blocks = total_rows // window

    def banded(earlier, current):
        joined = jnp.concatenate([earlier, current], axis=0).reshape(blocks + 1, window, kv_count, head_size)
        return jnp.concatenate([joined[:-1], joined[1:]], axis=1)
    band_keys = banded(prior_keys, key_heads)
    band_values = banded(prior_values, value_heads)
    query_blocks = query_heads.reshape(blocks, window, kv_count, group_size, head_size)
    scores = jnp.einsum('nqhgd,nkhd->nhgqk', query_blocks.astype(jnp.float32), band_keys.astype(jnp.float32)) / math.sqrt(head_size)
    query_index = jnp.arange(window, dtype=jnp.int32)[:, None]
    key_index = jnp.arange(2 * window, dtype=jnp.int32)[None, :]
    distance = query_index + window - key_index
    block_start = first_position + jnp.arange(blocks, dtype=jnp.int32)[:, None, None] * window
    allowed = (distance >= 0) & (distance < window) & (block_start - window + key_index >= 0)
    scores = jnp.where(allowed[:, None, None, :, :], scores, -jnp.inf)
    sink_grid = sink_logits.astype(jnp.float32).reshape(kv_count, group_size)[None, :, :, None, None]
    row_peak = jnp.maximum(lax.optimization_barrier(jnp.max(scores, axis=-1, keepdims=True)), sink_grid)
    shifted_exp = jnp.exp(scores - row_peak)
    denominator = lax.optimization_barrier(jnp.sum(shifted_exp, axis=-1, keepdims=True)) + jnp.exp(sink_grid - row_peak)
    probs = (shifted_exp / denominator).astype(jnp.bfloat16)
    attended = jnp.einsum('nhgqk,nkhd->nqhgd', probs.astype(jnp.float32), band_values.astype(jnp.float32))
    return attended.astype(jnp.bfloat16).reshape(total_rows, kv_count * group_size * head_size)

def reference(mixer_input, expert_input, gain_mixer, gain_expert, query_weight, key_weight, value_weight, sink_logits, output_weight, expert_choice, route_weights, expert_gate, expert_up, expert_down, shared_gate, shared_up, shared_down):
    head_block = HEADS * HEAD_DIM // N_TP

    def one_sequence(seq_rows):
        normed = rms_scale(seq_rows, gain_mixer)
        queries = jnp.dot(normed, query_weight, preferred_element_type=jnp.float32).astype(jnp.bfloat16)
        key_rows = jnp.dot(normed, key_weight, preferred_element_type=jnp.float32).astype(jnp.bfloat16)
        value_rows = jnp.dot(normed, value_weight, preferred_element_type=jnp.float32).astype(jnp.bfloat16)
        positions = jnp.arange(SEQ_LEN, dtype=jnp.float32)
        angles = positions[:, None] * frequencies(HEAD_DIM)[None, :]
        rot_queries = rotate(queries.reshape(SEQ_LEN, HEADS, HEAD_DIM), angles)
        rot_keys = rotate(key_rows.reshape(SEQ_LEN, KV_HEADS, HEAD_DIM), angles)
        value_heads = value_rows.reshape(SEQ_LEN, KV_HEADS, HEAD_DIM)
        empty_rows = jnp.zeros((WINDOW, KV_HEADS, HEAD_DIM), jnp.bfloat16)
        attended = attend(rot_queries, rot_keys, value_heads, empty_rows, empty_rows, 0, sink_logits)
        mixed_sum = jnp.zeros((SEQ_LEN, D), jnp.float32)
        for slice_index in range(N_TP):
            low_edge = slice_index * head_block
            mixed_sum = mixed_sum + rounded(jnp.dot(attended[:, low_edge:low_edge + head_block], output_weight[low_edge:low_edge + head_block], preferred_element_type=jnp.float32))
        return mixed_sum.astype(jnp.bfloat16)
    mixer_output = lax.map(one_sequence, mixer_input.reshape(SEQS, SEQ_LEN, D)).reshape(TOKENS_A, D)
    normed_rows = rms_scale(expert_input, gain_expert)
    padded_rows = jnp.concatenate([normed_rows, jnp.zeros((1, D), jnp.bfloat16)], axis=0)
    block_count = TOKENS_B // TOK_B_DEV
    assigned = TOK_B_DEV * TOP
    picked_experts = expert_choice.reshape(block_count, assigned)
    onehot = (picked_experts[:, :, None] == jnp.arange(EXPERTS, dtype=jnp.int32)[None, None, :]).astype(jnp.int32)
    slot_ranks = lax.optimization_barrier(jnp.sum(jnp.cumsum(onehot, axis=1) * onehot, axis=-1)) - 1
    block_ids = jnp.arange(block_count, dtype=jnp.int32)[:, None]
    slot_index = (picked_experts * block_count + block_ids) * CAP + slot_ranks
    token_owner = block_ids * TOK_B_DEV + jnp.arange(assigned, dtype=jnp.int32)[None, :] // TOP
    slot_table = jnp.full((EXPERTS * block_count * CAP,), TOKENS_B, jnp.int32).at[slot_index.reshape(-1)].set(token_owner.reshape(-1).astype(jnp.int32))
    weight_table = jnp.zeros((EXPERTS * block_count * CAP,), jnp.float32).at[slot_index.reshape(-1)].set(route_weights.reshape(-1).astype(jnp.float32))
    ff_block = EXPERT_FF // N_TP

    def one_expert(carry, inputs):
        index_row, weight_row, gate_matrix, up_matrix, down_matrix = inputs
        chosen_rows = padded_rows[index_row]
        gate_values = jnp.dot(chosen_rows, gate_matrix, preferred_element_type=jnp.float32)
        up_values = jnp.dot(chosen_rows, up_matrix, preferred_element_type=jnp.float32)
        hidden = (jax.nn.silu(gate_values) * up_values).astype(jnp.bfloat16)
        result = jnp.zeros((chosen_rows.shape[0], D), jnp.float32)
        for slice_index in range(N_TP):
            low_edge = slice_index * ff_block
            result = result + rounded(jnp.dot(hidden[:, low_edge:low_edge + ff_block], down_matrix[low_edge:low_edge + ff_block], preferred_element_type=jnp.float32))
        return (carry.at[index_row].add(result * weight_row[:, None]), None)
    routed, unused = lax.scan(one_expert, jnp.zeros((TOKENS_B + 1, D), jnp.float32), (slot_table.reshape(EXPERTS, block_count * CAP), weight_table.reshape(EXPERTS, block_count * CAP), expert_gate, expert_up, expert_down))
    shared_gate_values = jnp.dot(normed_rows, shared_gate, preferred_element_type=jnp.float32)
    shared_up_values = jnp.dot(normed_rows, shared_up, preferred_element_type=jnp.float32)
    shared_hidden = (jax.nn.silu(shared_gate_values) * shared_up_values).astype(jnp.bfloat16)
    shared_block = SHARED_FF // N_TP
    shared_result = jnp.zeros((TOKENS_B, D), jnp.float32)
    for slice_index in range(N_TP):
        low_edge = slice_index * shared_block
        shared_result = shared_result + rounded(jnp.dot(shared_hidden[:, low_edge:low_edge + shared_block], shared_down[low_edge:low_edge + shared_block], preferred_element_type=jnp.float32))
    expert_output = (routed[:TOKENS_B] + shared_result).astype(jnp.bfloat16)
    return (mixer_output, expert_output)
```

```python
import math

import jax
import jax.numpy as jnp
from jax import lax
from jax.experimental import pallas as pl
from jax.experimental.pallas import tpu as pltpu
from jax.sharding import PartitionSpec as P

HEAD_DIM = 64
WINDOW = 128
SEQS = 1
CHUNKS = 2


norm_eps = 1e-06
rope_base = 500000.0


def from_behind(value, axis, steps):
    count = lax.axis_size(axis)
    first, last = (max(0, -steps), min(count, count - steps))
    return lax.ppermute(value, axis, [(source, source + steps) for source in range(first, last)])


def rms_scale(matrix, scaling):
    widened = matrix.astype(jnp.float32)
    scaled = widened * lax.rsqrt(jnp.mean(widened * widened, axis=-1, keepdims=True) + norm_eps)
    return (scaled * scaling).astype(jnp.bfloat16)


def frequencies(head_size):
    half_steps = jnp.arange(head_size // 2, dtype=jnp.float32)
    return rope_base ** (-(2.0 * half_steps) / head_size)


def rotate(heads, angles):
    middle = heads.shape[-1] // 2
    widened = heads.astype(jnp.float32)
    cosine = jnp.cos(angles)[:, None, :]
    sine_val = jnp.sin(angles)[:, None, :]
    leading = widened[..., :middle]
    trailing = widened[..., middle:]
    turned = jnp.concatenate(
        [leading * cosine - trailing * sine_val, trailing * cosine + leading * sine_val], axis=-1
    )
    return turned.astype(jnp.bfloat16)


def attend(
    query_heads, key_heads, value_heads, prior_keys, prior_values, first_position, sink_logits
):
    window = prior_keys.shape[0]
    total_rows, kv_count, head_size = key_heads.shape
    group_size = query_heads.shape[1] // kv_count
    blocks = total_rows // window

    def banded(earlier, current):
        joined = jnp.concatenate([earlier, current], axis=0).reshape(
            blocks + 1, window, kv_count, head_size
        )
        return jnp.concatenate([joined[:-1], joined[1:]], axis=1)

    band_keys = banded(prior_keys, key_heads)
    band_values = banded(prior_values, value_heads)
    query_blocks = query_heads.reshape(blocks, window, kv_count, group_size, head_size)
    scores = jnp.einsum(
        "nqhgd,nkhd->nhgqk", query_blocks, band_keys, preferred_element_type=jnp.float32
    ) / math.sqrt(head_size)
    query_index = jnp.arange(window, dtype=jnp.int32)[:, None]
    key_index = jnp.arange(2 * window, dtype=jnp.int32)[None, :]
    distance = query_index + window - key_index
    block_start = first_position + jnp.arange(blocks, dtype=jnp.int32)[:, None, None] * window
    allowed = (distance >= 0) & (distance < window) & (block_start - window + key_index >= 0)
    scores = jnp.where(allowed[:, None, None, :, :], scores, -jnp.inf)
    sink_grid = sink_logits.reshape(kv_count, group_size)[None, :, :, None, None]
    row_peak = jnp.maximum(jnp.max(scores, axis=-1, keepdims=True), sink_grid)
    shifted_exp = jnp.exp(scores - row_peak)
    denominator = jnp.sum(shifted_exp, axis=-1, keepdims=True) + jnp.exp(sink_grid - row_peak)
    probs = (shifted_exp / denominator).astype(jnp.bfloat16)
    attended = jnp.einsum(
        "nhgqk,nkhd->nqhgd", probs, band_values, preferred_element_type=jnp.float32
    )
    return attended.astype(jnp.bfloat16).reshape(total_rows, kv_count * group_size * head_size)


def dispatch_kernel(capacity, experts):
    def body(rank_ref, rows_ref, gain_ref, choice_ref, out_ref, pick_ref):
        rows = rows_ref[...].astype(jnp.float32)
        tokens = rows.shape[0]
        slots = experts * capacity
        scale = lax.rsqrt(jnp.mean(rows * rows, axis=-1, keepdims=True) + norm_eps)
        normed = (rows * scale * gain_ref[...]).astype(jnp.bfloat16)
        first = choice_ref[:, 0:1]
        second = choice_ref[:, 1:2]
        expert = lax.broadcasted_iota(jnp.int32, (tokens, experts), 1)
        named = jnp.where((first == expert) | (second == expert), 1.0, 0.0).astype(jnp.bfloat16)
        row = lax.broadcasted_iota(jnp.int32, (tokens, tokens), 0)
        col = lax.broadcasted_iota(jnp.int32, (tokens, tokens), 1)
        earlier = jnp.where(row > col, 1.0, 0.0).astype(jnp.bfloat16)
        ranks = jnp.dot(earlier, named, preferred_element_type=jnp.float32)
        spread_e = lax.broadcasted_iota(jnp.int32, (experts, slots), 0)
        spread_s = lax.broadcasted_iota(jnp.int32, (experts, slots), 1)
        spread = jnp.where(spread_s // capacity == spread_e, 1.0, 0.0).astype(jnp.bfloat16)
        slot_rank = jnp.dot(ranks.astype(jnp.bfloat16), spread, preferred_element_type=jnp.float32)
        slot = lax.broadcasted_iota(jnp.int32, (tokens, slots), 1)
        fits = slot_rank.astype(jnp.int32) == slot % capacity
        owner = slot // capacity
        pick_first = jnp.where((owner == first) & fits, 1.0, 0.0).astype(jnp.bfloat16)
        pick_second = jnp.where((owner == second) & fits, 1.0, 0.0).astype(jnp.bfloat16)
        pick_ref[0] = pick_first
        pick_ref[1] = pick_second
        out_ref[...] = lax.dot_general(
            pick_first + pick_second,
            normed,
            (((0,), (0,)), ((), ())),
            preferred_element_type=jnp.float32,
        ).astype(jnp.bfloat16)

    return body


def dispatched(rank, rows, gain, choice, tokens, capacity, experts):
    width = rows.shape[1]
    slots = experts * capacity
    return pl.pallas_call(
        dispatch_kernel(capacity, experts),
        grid_spec=pltpu.PrefetchScalarGridSpec(
            num_scalar_prefetch=1,
            grid=(1,),
            in_specs=[
                pl.BlockSpec((tokens, width), lambda i, r: (r[0], 0)),
                pl.BlockSpec((1, width), lambda i, r: (0, 0)),
                pl.BlockSpec((tokens, 2), lambda i, r: (r[0], 0)),
            ],
            out_specs=[
                pl.BlockSpec((slots, width), lambda i, r: (0, 0)),
                pl.BlockSpec((2, tokens, slots), lambda i, r: (0, 0, 0)),
            ],
        ),
        out_shape=[
            jax.ShapeDtypeStruct((slots, width), jnp.bfloat16),
            jax.ShapeDtypeStruct((2, tokens, slots), jnp.bfloat16),
        ],
        name="dispatch",
    )(rank, rows, gain, choice)


def hidden_body(rows_ref, gate_ref, up_ref, out_ref):
    gate = jnp.dot(rows_ref[...], gate_ref[0], preferred_element_type=jnp.float32)
    up = jnp.dot(rows_ref[...], up_ref[0], preferred_element_type=jnp.float32)
    out_ref[...] = (gate / (1.0 + jnp.exp(-gate)) * up).astype(jnp.bfloat16)


def expert_hidden(rows, gate, up):
    slots, width = rows.shape
    parts, _, units = gate.shape
    return pl.pallas_call(
        hidden_body,
        grid=(parts,),
        in_specs=[
            pl.BlockSpec((slots, width), lambda i: (0, 0)),
            pl.BlockSpec((1, width, units), lambda i: (i, 0, 0)),
            pl.BlockSpec((1, width, units), lambda i: (i, 0, 0)),
        ],
        out_specs=pl.BlockSpec((slots, units), lambda i: (0, i)),
        out_shape=jax.ShapeDtypeStruct((slots, parts * units), jnp.bfloat16),
        name="hidden",
    )(rows, gate, up)


def combine_body(rank_ref, pick_ref, weight_ref, shared_ref, *rest):
    parts = rest[:-1]
    out_ref = rest[-1]
    first = weight_ref[:, 0:1]
    second = weight_ref[:, 1:2]
    at = 0
    for part in parts:
        returned = part[...]
        span = returned.shape[1]
        total = first * jnp.dot(pick_ref[0], returned, preferred_element_type=jnp.float32)
        total = total + second * jnp.dot(pick_ref[1], returned, preferred_element_type=jnp.float32)
        total = total + shared_ref[:, at : at + span].astype(jnp.float32)
        out_ref[:, at : at + span] = total.astype(jnp.bfloat16)
        at += span


def combined(rank, pick, weights, shared, parts):
    tokens, width = shared.shape
    whole = lambda shape: pl.BlockSpec(shape, lambda i, r: (0,) * len(shape))
    return pl.pallas_call(
        combine_body,
        grid_spec=pltpu.PrefetchScalarGridSpec(
            num_scalar_prefetch=1,
            grid=(1,),
            in_specs=[
                whole(pick.shape),
                pl.BlockSpec((tokens, 2), lambda i, r: (r[0], 0)),
                whole(shared.shape),
                *[whole(part.shape) for part in parts],
            ],
            out_specs=whole((tokens, width)),
        ),
        out_shape=jax.ShapeDtypeStruct((tokens, width), jnp.bfloat16),
        name="combine",
    )(rank, pick, weights, shared, *parts)


def local(
    mixer_input,
    expert_input,
    gain_mixer,
    gain_expert,
    query_weight,
    key_weight,
    value_weight,
    sink_logits,
    output_weight,
    expert_choice,
    route_weights,
    expert_gate,
    expert_up,
    expert_down,
    shared_gate,
    shared_up,
    shared_down,
):
    tp_count = lax.axis_size("tp")
    ep_count = lax.axis_size("ep")
    tp_rank = lax.axis_index("tp")
    rank = tp_rank.astype(jnp.int32).reshape(1)
    group_rows, model_width = mixer_input.shape
    group_tokens = expert_input.shape[0]
    own_tokens = group_tokens // tp_count
    top_count = expert_choice.shape[1]
    experts_all = ep_count
    capacity = 2 * own_tokens * top_count // experts_all

    gate_all = lax.all_gather(expert_gate[0], "tp", axis=0)
    up_all = lax.all_gather(expert_up[0], "tp", axis=0)
    span = model_width // CHUNKS
    down_parts = [
        lax.all_gather(expert_down[0][:, at * span : (at + 1) * span], "tp", axis=0, tiled=True)
        for at in range(CHUNKS)
    ]

    outgoing, pick = dispatched(
        rank, expert_input, gain_expert[None, :], expert_choice, own_tokens, capacity, experts_all
    )
    arrived = lax.all_to_all(
        outgoing.reshape(experts_all, capacity, model_width),
        "ep",
        split_axis=0,
        concat_axis=0,
        tiled=True,
    ).reshape(experts_all * capacity, model_width)

    normed = rms_scale(mixer_input, gain_mixer)
    queries = jnp.dot(normed, query_weight, preferred_element_type=jnp.float32).astype(jnp.bfloat16)
    key_rows = jnp.dot(normed, key_weight, preferred_element_type=jnp.float32).astype(jnp.bfloat16)
    value_rows = jnp.dot(normed, value_weight, preferred_element_type=jnp.float32).astype(
        jnp.bfloat16
    )
    first_position = lax.axis_index("ep") % (ep_count // SEQS) * group_rows
    positions = (first_position + jnp.arange(group_rows, dtype=jnp.int32)).astype(jnp.float32)
    angles = positions[:, None] * frequencies(HEAD_DIM)[None, :]
    rot_queries = rotate(queries.reshape(group_rows, -1, HEAD_DIM), angles)
    rot_keys = rotate(key_rows.reshape(group_rows, -1, HEAD_DIM), angles)
    key_width = key_rows.shape[1]
    tail_start = group_rows - WINDOW
    tail_pair = jnp.concatenate(
        [rot_keys.reshape(group_rows, key_width)[tail_start:], value_rows[tail_start:]], axis=1
    )
    earlier_pair = from_behind(tail_pair, "ep", 1)
    prior_keys = earlier_pair[:, :key_width].reshape(WINDOW, -1, HEAD_DIM)
    prior_values = earlier_pair[:, key_width:].reshape(WINDOW, -1, HEAD_DIM)
    attended = attend(
        rot_queries,
        rot_keys,
        value_rows.reshape(group_rows, -1, HEAD_DIM),
        prior_keys,
        prior_values,
        first_position,
        sink_logits,
    )
    mixer_part = jnp.dot(attended, output_weight, preferred_element_type=jnp.float32)
    mixer_output = lax.psum_scatter(
        mixer_part.astype(jnp.bfloat16), "tp", scatter_dimension=0, tiled=True
    )

    normed_rows = rms_scale(expert_input, gain_expert)
    gate_values = jnp.dot(normed_rows, shared_gate, preferred_element_type=jnp.float32)
    up_values = jnp.dot(normed_rows, shared_up, preferred_element_type=jnp.float32)
    hidden = (jax.nn.silu(gate_values) * up_values).astype(jnp.bfloat16)
    shared_part = lax.psum_scatter(
        jnp.dot(hidden, shared_down, preferred_element_type=jnp.float32).astype(jnp.bfloat16),
        "tp",
        scatter_dimension=0,
        tiled=True,
    )

    routed_hidden = expert_hidden(arrived, gate_all, up_all)
    returned = []
    for down in down_parts:
        result = jnp.dot(routed_hidden, down, preferred_element_type=jnp.float32).astype(jnp.bfloat16)
        returned.append(
            lax.all_to_all(
                result.reshape(experts_all, capacity, -1),
                "ep",
                split_axis=0,
                concat_axis=0,
                tiled=True,
            ).reshape(experts_all * capacity, -1)
        )
    expert_output = combined(rank, pick, route_weights, shared_part, returned)
    return (mixer_output, expert_output)


def solution(mesh):
    placed = (
        P("ep", None),
        P("ep", None),
        P(),
        P(),
        P(None, "tp"),
        P(None, "tp"),
        P(None, "tp"),
        P("tp"),
        P("tp", None),
        P("ep", None),
        P("ep", None),
        P("ep", None, "tp"),
        P("ep", None, "tp"),
        P("ep", "tp", None),
        P(None, "tp"),
        P(None, "tp"),
        P("tp", None),
    )
    return jax.shard_map(
        local,
        mesh=mesh,
        in_specs=placed,
        out_specs=(P(("ep", "tp"), None), P(("ep", "tp"), None)),
        check_vma=False,
    )
```

```python
import math

import jax
import jax.numpy as jnp
from jax import lax
from jax.experimental import pallas as pl
from jax.experimental.pallas import tpu as pltpu
from jax.sharding import PartitionSpec as P


HEAD_DIM = 64
WINDOW = 128
SEQS = 1
PIECES = ((256, 256), (768, 768))


norm_eps = 1e-06
rope_base = 500000.0


def from_behind(value, axis, steps):
    count = lax.axis_size(axis)
    first, last = (max(0, -steps), min(count, count - steps))
    return lax.ppermute(value, axis, [(source, source + steps) for source in range(first, last)])


def shifted(value, steps):
    count = lax.axis_size("tp")
    return lax.ppermute(value, "tp", [(at, (at + steps) % count) for at in range(count)])


def crossed(value, mask):
    return lax.ppermute(value, "tp", [(at, at ^ mask) for at in range(lax.axis_size("tp"))])


def exchanged(rows, experts):
    slots, width = rows.shape
    return lax.all_to_all(
        rows.reshape(experts, slots // experts, width),
        "ep",
        split_axis=0,
        concat_axis=0,
        tiled=True,
    ).reshape(slots, width)


def halved_sum(rows, weight, own_rows, mask):
    rank = lax.axis_index("tp")
    other = mask ^ 2

    def product(*masks):
        blocks = [
            lax.dynamic_slice_in_dim(rows, (rank ^ each) * own_rows, own_rows, 0) for each in masks
        ]
        joined = jnp.concatenate(blocks, axis=0)
        return jnp.dot(joined, weight, preferred_element_type=jnp.float32).astype(jnp.bfloat16)

    got = crossed(product(mask, 2), mask)
    kept = product(0, other)
    half = kept.astype(jnp.float32) + got.astype(jnp.float32)
    last = crossed(half[own_rows:].astype(jnp.bfloat16), other)
    return half[:own_rows] + last.astype(jnp.float32)


def rms_scale(matrix, scaling):
    widened = matrix.astype(jnp.float32)
    scaled = widened * lax.rsqrt(jnp.mean(widened * widened, axis=-1, keepdims=True) + norm_eps)
    return (scaled * scaling).astype(jnp.bfloat16)


def frequencies(head_size):
    half_steps = jnp.arange(head_size // 2, dtype=jnp.float32)
    return rope_base ** (-(2.0 * half_steps) / head_size)


def rotate(heads, angles):
    middle = heads.shape[-1] // 2
    widened = heads.astype(jnp.float32)
    cosine = jnp.cos(angles)[:, None, :]
    sine_val = jnp.sin(angles)[:, None, :]
    leading = widened[..., :middle]
    trailing = widened[..., middle:]
    turned = jnp.concatenate(
        [leading * cosine - trailing * sine_val, trailing * cosine + leading * sine_val], axis=-1
    )
    return turned.astype(jnp.bfloat16)


def attend(
    query_heads, key_heads, value_heads, prior_keys, prior_values, first_position, sink_logits
):
    window = prior_keys.shape[0]
    total_rows, kv_count, head_size = key_heads.shape
    group_size = query_heads.shape[1] // kv_count
    blocks = total_rows // window

    def banded(earlier, current):
        joined = jnp.concatenate([earlier, current], axis=0).reshape(
            blocks + 1, window, kv_count, head_size
        )
        return jnp.concatenate([joined[:-1], joined[1:]], axis=1)

    band_keys = banded(prior_keys, key_heads)
    band_values = banded(prior_values, value_heads)
    query_blocks = query_heads.reshape(blocks, window, kv_count, group_size, head_size)
    scores = jnp.einsum(
        "nqhgd,nkhd->nhgqk", query_blocks, band_keys, preferred_element_type=jnp.float32
    ) / math.sqrt(head_size)
    query_index = jnp.arange(window, dtype=jnp.int32)[:, None]
    key_index = jnp.arange(2 * window, dtype=jnp.int32)[None, :]
    distance = query_index + window - key_index
    block_start = first_position + jnp.arange(blocks, dtype=jnp.int32)[:, None, None] * window
    allowed = (distance >= 0) & (distance < window) & (block_start - window + key_index >= 0)
    scores = jnp.where(allowed[:, None, None, :, :], scores, -jnp.inf)
    sink_grid = sink_logits.reshape(kv_count, group_size)[None, :, :, None, None]
    row_peak = jnp.maximum(jnp.max(scores, axis=-1, keepdims=True), sink_grid)
    shifted_exp = jnp.exp(scores - row_peak)
    denominator = jnp.sum(shifted_exp, axis=-1, keepdims=True) + jnp.exp(sink_grid - row_peak)
    probs = (shifted_exp / denominator).astype(jnp.bfloat16)
    attended = jnp.einsum(
        "nhgqk,nkhd->nqhgd", probs, band_values, preferred_element_type=jnp.float32
    )
    return attended.astype(jnp.bfloat16).reshape(total_rows, kv_count * group_size * head_size)


def dispatch_kernel(capacity, experts):
    def body(rank_ref, rows_ref, gain_ref, choice_ref, out_ref, pick_ref):
        rows = rows_ref[...].astype(jnp.float32)
        tokens = rows.shape[0]
        slots = experts * capacity
        scale = lax.rsqrt(jnp.mean(rows * rows, axis=-1, keepdims=True) + norm_eps)
        normed = (rows * scale * gain_ref[...]).astype(jnp.bfloat16)
        first = choice_ref[:, 0:1]
        second = choice_ref[:, 1:2]
        expert = lax.broadcasted_iota(jnp.int32, (tokens, experts), 1)
        named = jnp.where((first == expert) | (second == expert), 1.0, 0.0).astype(jnp.bfloat16)
        row = lax.broadcasted_iota(jnp.int32, (tokens, tokens), 0)
        col = lax.broadcasted_iota(jnp.int32, (tokens, tokens), 1)
        earlier = jnp.where(row > col, 1.0, 0.0).astype(jnp.bfloat16)
        ranks = jnp.dot(earlier, named, preferred_element_type=jnp.float32)
        spread_e = lax.broadcasted_iota(jnp.int32, (experts, slots), 0)
        spread_s = lax.broadcasted_iota(jnp.int32, (experts, slots), 1)
        spread = jnp.where(spread_s // capacity == spread_e, 1.0, 0.0).astype(jnp.bfloat16)
        slot_rank = jnp.dot(ranks.astype(jnp.bfloat16), spread, preferred_element_type=jnp.float32)
        slot = lax.broadcasted_iota(jnp.int32, (tokens, slots), 1)
        fits = slot_rank.astype(jnp.int32) == slot % capacity
        owner = slot // capacity
        pick_first = jnp.where((owner == first) & fits, 1.0, 0.0).astype(jnp.bfloat16)
        pick_second = jnp.where((owner == second) & fits, 1.0, 0.0).astype(jnp.bfloat16)
        pick_ref[0] = pick_first
        pick_ref[1] = pick_second
        out_ref[...] = lax.dot_general(
            pick_first + pick_second,
            normed,
            (((0,), (0,)), ((), ())),
            preferred_element_type=jnp.float32,
        ).astype(jnp.bfloat16)

    return body


def dispatched(rank, rows, gain, choice, tokens, capacity, experts):
    width = rows.shape[1]
    slots = experts * capacity
    return pl.pallas_call(
        dispatch_kernel(capacity, experts),
        grid_spec=pltpu.PrefetchScalarGridSpec(
            num_scalar_prefetch=1,
            grid=(1,),
            in_specs=[
                pl.BlockSpec((tokens, width), lambda i, r: (r[0], 0)),
                pl.BlockSpec((1, width), lambda i, r: (0, 0)),
                pl.BlockSpec((tokens, 2), lambda i, r: (r[0], 0)),
            ],
            out_specs=[
                pl.BlockSpec((slots, width), lambda i, r: (0, 0)),
                pl.BlockSpec((2, tokens, slots), lambda i, r: (0, 0, 0)),
            ],
        ),
        out_shape=[
            jax.ShapeDtypeStruct((slots, width), jnp.bfloat16),
            jax.ShapeDtypeStruct((2, tokens, slots), jnp.bfloat16),
        ],
        name="dispatch",
    )(rank, rows, gain, choice)


def hidden_body(rows_ref, *refs):
    out_ref = refs[-1]
    weights = refs[:-1]
    at = 0
    for gate_ref, up_ref in zip(weights[0::2], weights[1::2]):
        units = gate_ref.shape[1]
        gate = jnp.dot(rows_ref[...], gate_ref[...], preferred_element_type=jnp.float32)
        up = jnp.dot(rows_ref[...], up_ref[...], preferred_element_type=jnp.float32)
        out_ref[:, at : at + units] = (gate / (1.0 + jnp.exp(-gate)) * up).astype(jnp.bfloat16)
        at += units


def expert_hidden(rows, pairs, steps=2):
    slots, width = rows.shape
    units = pairs[0][0].shape[1]
    block = slots // steps
    flat = [matrix for pair in pairs for matrix in pair]
    return pl.pallas_call(
        hidden_body,
        grid=(steps,),
        in_specs=[pl.BlockSpec((block, width), lambda i: (i, 0))]
        + [pl.BlockSpec((width, units), lambda i: (0, 0))] * len(flat),
        out_specs=pl.BlockSpec((block, len(pairs) * units), lambda i: (i, 0)),
        out_shape=jax.ShapeDtypeStruct((slots, len(pairs) * units), jnp.bfloat16),
        name="hidden",
    )(rows, *flat)


def down_body(hidden_ref, *refs):
    out_ref = refs[-1]
    weights = refs[:-1]
    slices = 4
    units = weights[0].shape[0]
    at = 0
    for piece in range(len(weights) // slices):
        group = weights[piece * slices : (piece + 1) * slices]
        span = group[0].shape[1]
        total = 0.0
        for index, weight in enumerate(group):
            total = total + jnp.dot(
                hidden_ref[:, index * units : (index + 1) * units],
                weight[...],
                preferred_element_type=jnp.float32,
            )
        out_ref[:, at : at + span] = total.astype(jnp.bfloat16)
        at += span


def expert_result(hidden, groups, steps=2):
    slots, units_all = hidden.shape
    block = slots // steps
    flat = [matrix for group in groups for matrix in group]
    width = sum(group[0].shape[1] for group in groups)
    return pl.pallas_call(
        down_body,
        grid=(steps,),
        in_specs=[pl.BlockSpec((block, units_all), lambda i: (i, 0))]
        + [pl.BlockSpec(matrix.shape, lambda i: (0, 0)) for matrix in flat],
        out_specs=pl.BlockSpec((block, width), lambda i: (i, 0)),
        out_shape=jax.ShapeDtypeStruct((slots, width), jnp.bfloat16),
        name="down",
    )(hidden, *flat)


def combine_body(rank_ref, pick_ref, weight_ref, shared_ref, *rest):
    parts = rest[:-1]
    out_ref = rest[-1]
    first = weight_ref[:, 0:1]
    second = weight_ref[:, 1:2]
    at = 0
    for part in parts:
        returned = part[...]
        span = returned.shape[1]
        total = first * jnp.dot(pick_ref[0], returned, preferred_element_type=jnp.float32)
        total = total + second * jnp.dot(pick_ref[1], returned, preferred_element_type=jnp.float32)
        total = total + shared_ref[:, at : at + span].astype(jnp.float32)
        out_ref[:, at : at + span] = total.astype(jnp.bfloat16)
        at += span


def combined(rank, pick, weights, shared, parts):
    tokens, width = shared.shape
    whole = lambda shape: pl.BlockSpec(shape, lambda i, r: (0,) * len(shape))
    return pl.pallas_call(
        combine_body,
        grid_spec=pltpu.PrefetchScalarGridSpec(
            num_scalar_prefetch=1,
            grid=(1,),
            in_specs=[
                whole(pick.shape),
                pl.BlockSpec((tokens, 2), lambda i, r: (r[0], 0)),
                whole(shared.shape),
                *[whole(part.shape) for part in parts],
            ],
            out_specs=whole((tokens, width)),
        ),
        out_shape=jax.ShapeDtypeStruct((tokens, width), jnp.bfloat16),
        name="combine",
    )(rank, pick, weights, shared, *parts)


def both(
    mixer_input,
    expert_input,
    gain_mixer,
    gain_expert,
    query_weight,
    key_weight,
    value_weight,
    sink_logits,
    output_weight,
    expert_choice,
    route_weights,
    expert_gate,
    expert_up,
    expert_down,
    shared_gate,
    shared_up,
    shared_down,
):
    tp_count = lax.axis_size("tp")
    ep_count = lax.axis_size("ep")
    tp_rank = lax.axis_index("tp")
    rank = tp_rank.astype(jnp.int32).reshape(1)
    group_rows, _ = mixer_input.shape
    group_tokens = expert_input.shape[0]
    own_tokens = group_tokens // tp_count
    top_count = expert_choice.shape[1]
    experts_all = ep_count
    capacity = 2 * own_tokens * top_count // experts_all

    gate, up, down = expert_gate[0], expert_up[0], expert_down[0]
    gate_left, gate_right = shifted(gate, 1), shifted(gate, -1)
    up_left, up_right = shifted(up, 1), shifted(up, -1)
    gate_far, up_far = shifted(gate_left, 1), shifted(up_right, -1)
    chunks = []
    at = 0
    for spans in PIECES:
        groups = []
        for index, span in enumerate(spans):
            piece = down[:, at : at + span]
            at += span
            left, right = shifted(piece, 1), shifted(piece, -1)
            if index == 0:
                far = shifted(left, 1)
            else:
                far = shifted(right, -1)
            groups.append((piece, left, right, far))
        chunks.append(groups)

    outgoing, pick = dispatched(
        rank, expert_input, gain_expert[None, :], expert_choice, own_tokens, capacity, experts_all
    )
    arrived = exchanged(outgoing, experts_all)

    normed = rms_scale(mixer_input, gain_mixer)
    queries = jnp.dot(normed, query_weight, preferred_element_type=jnp.float32).astype(jnp.bfloat16)
    key_rows = jnp.dot(normed, key_weight, preferred_element_type=jnp.float32).astype(jnp.bfloat16)
    value_rows = jnp.dot(normed, value_weight, preferred_element_type=jnp.float32).astype(
        jnp.bfloat16
    )
    first_position = lax.axis_index("ep") % (ep_count // SEQS) * group_rows
    positions = (first_position + jnp.arange(group_rows, dtype=jnp.int32)).astype(jnp.float32)
    angles = positions[:, None] * frequencies(HEAD_DIM)[None, :]
    rot_queries = rotate(queries.reshape(group_rows, -1, HEAD_DIM), angles)
    rot_keys = rotate(key_rows.reshape(group_rows, -1, HEAD_DIM), angles)
    key_width = key_rows.shape[1]
    tail_start = group_rows - WINDOW
    tail_pair = jnp.concatenate(
        [rot_keys.reshape(group_rows, key_width)[tail_start:], value_rows[tail_start:]], axis=1
    )
    earlier_pair = from_behind(tail_pair, "ep", 1)
    prior_keys = earlier_pair[:, :key_width].reshape(WINDOW, -1, HEAD_DIM)
    prior_values = earlier_pair[:, key_width:].reshape(WINDOW, -1, HEAD_DIM)
    attended = attend(
        rot_queries,
        rot_keys,
        value_rows.reshape(group_rows, -1, HEAD_DIM),
        prior_keys,
        prior_values,
        first_position,
        sink_logits,
    )
    mixer_output = halved_sum(attended, output_weight, own_tokens, 1).astype(jnp.bfloat16)

    normed_rows = rms_scale(expert_input, gain_expert)
    gate_values = jnp.dot(normed_rows, shared_gate, preferred_element_type=jnp.float32)
    up_values = jnp.dot(normed_rows, shared_up, preferred_element_type=jnp.float32)
    hidden = (jax.nn.silu(gate_values) * up_values).astype(jnp.bfloat16)
    shared_part = halved_sum(hidden, shared_down, own_tokens, 3)

    routed_hidden = expert_hidden(
        arrived, [(gate, up), (gate_left, up_left), (gate_right, up_right), (gate_far, up_far)]
    )
    returned = []
    for groups in chunks:
        result = expert_result(routed_hidden, groups)
        returned.append(exchanged(result, experts_all))
    expert_output = combined(rank, pick, route_weights, shared_part, returned)
    return (mixer_output, expert_output)


def solution(mesh):
    placed = (
        P("ep", None),
        P("ep", None),
        P(),
        P(),
        P(None, "tp"),
        P(None, "tp"),
        P(None, "tp"),
        P("tp"),
        P("tp", None),
        P("ep", None),
        P("ep", None),
        P("ep", None, "tp"),
        P("ep", None, "tp"),
        P("ep", "tp", None),
        P(None, "tp"),
        P(None, "tp"),
        P("tp", None),
    )
    return jax.shard_map(
        both,
        mesh=mesh,
        in_specs=placed,
        out_specs=(P(("ep", "tp"), None), P(("ep", "tp"), None)),
        check_vma=False,
    )
```

```python
import math

import jax
import jax.numpy as jnp
from jax import lax
from jax.experimental import pallas as pl
from jax.experimental.pallas import tpu as pltpu
from jax.sharding import PartitionSpec as P


HEAD_DIM = 64
WINDOW = 128
SEQS = 1
SPANS = (768, 1280)


norm_eps = 1e-06
rope_base = 500000.0


def from_behind(value, axis, steps):
    count = lax.axis_size(axis)
    first, last = (max(0, -steps), min(count, count - steps))
    return lax.ppermute(value, axis, [(source, source + steps) for source in range(first, last)])


def shifted(value, steps):
    count = lax.axis_size("tp")
    return lax.ppermute(value, "tp", [(at, (at + steps) % count) for at in range(count)])


def crossed(value, mask):
    return lax.ppermute(value, "tp", [(at, at ^ mask) for at in range(lax.axis_size("tp"))])


def exchanged(rows, experts):
    slots, width = rows.shape
    return lax.all_to_all(
        rows.reshape(experts, slots // experts, width),
        "ep",
        split_axis=0,
        concat_axis=0,
        tiled=True,
    ).reshape(slots, width)


def halved_products(rows, weight, own_rows, mask):
    rank = lax.axis_index("tp")

    def product(*masks):
        blocks = [
            lax.dynamic_slice_in_dim(rows, (rank ^ each) * own_rows, own_rows, 0) for each in masks
        ]
        joined = jnp.concatenate(blocks, axis=0)
        return jnp.dot(joined, weight, preferred_element_type=jnp.float32).astype(jnp.bfloat16)

    return product(mask, 2), product(0, mask ^ 2)


def halved_sum(sent, kept, mask):
    own_rows = kept.shape[0] // 2
    got = crossed(sent, mask)
    half = kept.astype(jnp.float32) + got.astype(jnp.float32)
    last = crossed(half[own_rows:].astype(jnp.bfloat16), mask ^ 2)
    return half[:own_rows] + last.astype(jnp.float32)


def rms_scale(matrix, scaling):
    widened = matrix.astype(jnp.float32)
    scaled = widened * lax.rsqrt(jnp.mean(widened * widened, axis=-1, keepdims=True) + norm_eps)
    return (scaled * scaling).astype(jnp.bfloat16)


def frequencies(head_size):
    half_steps = jnp.arange(head_size // 2, dtype=jnp.float32)
    return rope_base ** (-(2.0 * half_steps) / head_size)


def rotate(heads, angles):
    middle = heads.shape[-1] // 2
    widened = heads.astype(jnp.float32)
    cosine = jnp.cos(angles)[:, None, :]
    sine_val = jnp.sin(angles)[:, None, :]
    leading = widened[..., :middle]
    trailing = widened[..., middle:]
    turned = jnp.concatenate(
        [leading * cosine - trailing * sine_val, trailing * cosine + leading * sine_val], axis=-1
    )
    return turned.astype(jnp.bfloat16)


def attend(
    query_heads, key_heads, value_heads, prior_keys, prior_values, first_position, sink_logits
):
    window = prior_keys.shape[0]
    total_rows, kv_count, head_size = key_heads.shape
    group_size = query_heads.shape[1] // kv_count
    blocks = total_rows // window

    def banded(earlier, current):
        joined = jnp.concatenate([earlier, current], axis=0).reshape(
            blocks + 1, window, kv_count, head_size
        )
        return jnp.concatenate([joined[:-1], joined[1:]], axis=1)

    band_keys = banded(prior_keys, key_heads)
    band_values = banded(prior_values, value_heads)
    query_blocks = query_heads.reshape(blocks, window, kv_count, group_size, head_size)
    scores = jnp.einsum(
        "nqhgd,nkhd->nhgqk", query_blocks, band_keys, preferred_element_type=jnp.float32
    ) / math.sqrt(head_size)
    query_index = jnp.arange(window, dtype=jnp.int32)[:, None]
    key_index = jnp.arange(2 * window, dtype=jnp.int32)[None, :]
    distance = query_index + window - key_index
    block_start = first_position + jnp.arange(blocks, dtype=jnp.int32)[:, None, None] * window
    allowed = (distance >= 0) & (distance < window) & (block_start - window + key_index >= 0)
    scores = jnp.where(allowed[:, None, None, :, :], scores, -jnp.inf)
    sink_grid = sink_logits.reshape(kv_count, group_size)[None, :, :, None, None]
    row_peak = jnp.maximum(jnp.max(scores, axis=-1, keepdims=True), sink_grid)
    shifted_exp = jnp.exp(scores - row_peak)
    denominator = jnp.sum(shifted_exp, axis=-1, keepdims=True) + jnp.exp(sink_grid - row_peak)
    probs = (shifted_exp / denominator).astype(jnp.bfloat16)
    attended = jnp.einsum(
        "nhgqk,nkhd->nqhgd", probs, band_values, preferred_element_type=jnp.float32
    )
    return attended.astype(jnp.bfloat16).reshape(total_rows, kv_count * group_size * head_size)


def dispatch_kernel(capacity, experts):
    def body(rank_ref, rows_ref, gain_ref, choice_ref, out_ref, pick_ref):
        rows = rows_ref[...].astype(jnp.float32)
        tokens = rows.shape[0]
        slots = experts * capacity
        scale = lax.rsqrt(jnp.mean(rows * rows, axis=-1, keepdims=True) + norm_eps)
        normed = (rows * scale * gain_ref[...]).astype(jnp.bfloat16)
        first = choice_ref[0:1, :]
        second = choice_ref[1:2, :]
        expert = lax.broadcasted_iota(jnp.int32, (experts, tokens), 0)
        named = jnp.where((first == expert) | (second == expert), 1.0, 0.0).astype(jnp.bfloat16)
        row = lax.broadcasted_iota(jnp.int32, (tokens, tokens), 0)
        col = lax.broadcasted_iota(jnp.int32, (tokens, tokens), 1)
        earlier = jnp.where(row < col, 1.0, 0.0).astype(jnp.bfloat16)
        ranks = jnp.dot(named, earlier, preferred_element_type=jnp.float32)
        slot_rank = jnp.broadcast_to(
            ranks.astype(jnp.int32)[:, None, :], (experts, capacity, tokens)
        ).reshape(slots, tokens)
        slot = lax.broadcasted_iota(jnp.int32, (slots, tokens), 0)
        fits = slot_rank == slot % capacity
        owner = slot // capacity
        pick_first = jnp.where((owner == first) & fits, 1.0, 0.0).astype(jnp.bfloat16)
        pick_second = jnp.where((owner == second) & fits, 1.0, 0.0).astype(jnp.bfloat16)
        pick_ref[0] = pick_first
        pick_ref[1] = pick_second
        out_ref[...] = jnp.dot(
            pick_first + pick_second, normed, preferred_element_type=jnp.float32
        ).astype(jnp.bfloat16)

    return body


def dispatched(rank, rows, gain, choice, tokens, capacity, experts):
    width = rows.shape[1]
    slots = experts * capacity
    return pl.pallas_call(
        dispatch_kernel(capacity, experts),
        grid_spec=pltpu.PrefetchScalarGridSpec(
            num_scalar_prefetch=1,
            grid=(1,),
            in_specs=[
                pl.BlockSpec((tokens, width), lambda i, r: (r[0], 0)),
                pl.BlockSpec((1, width), lambda i, r: (0, 0)),
                pl.BlockSpec((2, tokens), lambda i, r: (0, r[0])),
            ],
            out_specs=[
                pl.BlockSpec((slots, width), lambda i, r: (0, 0)),
                pl.BlockSpec((2, slots, tokens), lambda i, r: (0, 0, 0)),
            ],
        ),
        out_shape=[
            jax.ShapeDtypeStruct((slots, width), jnp.bfloat16),
            jax.ShapeDtypeStruct((2, slots, tokens), jnp.bfloat16),
        ],
        name="dispatch",
    )(rank, rows, gain, choice)


def hidden_body(rows_ref, *refs):
    count = len(refs) - 4
    sources, (out_ref, rows, held, sems) = refs[:count], refs[count:]
    units = held.shape[2] // 2
    copies = [pltpu.make_async_copy(rows_ref, rows, sems.at[count])]
    for at, source in enumerate(sources):
        place = held.at[at // 2, :, pl.ds(at % 2 * units, units)]
        copies.append(pltpu.make_async_copy(source, place, sems.at[at]))
    for copy in copies:
        copy.start()
    copies[0].wait()
    for index in range(held.shape[0]):
        copies[1 + 2 * index].wait()
        copies[2 + 2 * index].wait()
        both_values = jnp.dot(rows[...], held[index], preferred_element_type=jnp.float32)
        gate = both_values[:, :units]
        up = both_values[:, units:]
        out_ref[:, index * units : (index + 1) * units] = (
            gate / (1.0 + jnp.exp(-gate)) * up
        ).astype(jnp.bfloat16)


def expert_hidden(rows, pairs):
    slots, width = rows.shape
    units = pairs[0][0].shape[1]
    flat = [matrix for pair in pairs for matrix in pair]
    return pl.pallas_call(
        hidden_body,
        grid=(1,),
        in_specs=[pl.BlockSpec(memory_space=pl.ANY)] * (1 + len(flat)),
        out_specs=pl.BlockSpec((slots, len(pairs) * units), lambda i: (0, 0)),
        out_shape=jax.ShapeDtypeStruct((slots, len(pairs) * units), jnp.bfloat16),
        scratch_shapes=[
            pltpu.VMEM((slots, width), rows.dtype),
            pltpu.VMEM((len(pairs), width, 2 * units), rows.dtype),
            pltpu.SemaphoreType.DMA((len(flat) + 1,)),
        ],
    )(rows, *flat)


def down_body(near_ref, far_hidden_ref, *refs):
    out_ref = refs[-1]
    whole = refs[:3]
    far = refs[3:-1]
    units = whole[0].shape[0]
    at = 0
    for part in far:
        span = part.shape[1]
        total = jnp.dot(far_hidden_ref[...], part[...], preferred_element_type=jnp.float32)
        for index in range(3):
            total = total + jnp.dot(
                near_ref[:, index * units : (index + 1) * units],
                whole[index][:, at : at + span],
                preferred_element_type=jnp.float32,
            )
        out_ref[:, at : at + span] = total.astype(jnp.bfloat16)
        at += span


def expert_result(near, far, matrices, steps=2):
    slots = near.shape[0]
    block = slots // steps
    width = matrices[0].shape[1]
    by_rows = lambda columns: pl.BlockSpec((block, columns), lambda i: (i, 0))
    return pl.pallas_call(
        down_body,
        grid=(steps,),
        in_specs=[by_rows(near.shape[1]), by_rows(far.shape[1])]
        + [pl.BlockSpec(matrix.shape, lambda i: (0, 0)) for matrix in matrices],
        out_specs=by_rows(width),
        out_shape=jax.ShapeDtypeStruct((slots, width), jnp.bfloat16),
        name="down",
    )(near, far, *matrices)


def both(
    mixer_input,
    expert_input,
    gain_mixer,
    gain_expert,
    query_weight,
    key_weight,
    value_weight,
    sink_logits,
    output_weight,
    expert_choice,
    route_weights,
    expert_gate,
    expert_up,
    expert_down,
    shared_gate,
    shared_up,
    shared_down,
):
    tp_count = lax.axis_size("tp")
    ep_count = lax.axis_size("ep")
    tp_rank = lax.axis_index("tp")
    rank = tp_rank.astype(jnp.int32).reshape(1)
    group_rows, _ = mixer_input.shape
    group_tokens = expert_input.shape[0]
    own_tokens = group_tokens // tp_count
    top_count = expert_choice.shape[1]
    experts_all = ep_count
    capacity = 2 * own_tokens * top_count // experts_all

    gate, up, down = expert_gate[0], expert_up[0], expert_down[0]
    gate_left, gate_right = shifted(gate, 1), shifted(gate, -1)
    up_left, up_right = shifted(up, 1), shifted(up, -1)
    gate_far, up_far = shifted(gate_left, 1), shifted(up_right, -1)
    near_down = []
    at = 0
    for span in SPANS:
        piece = down[:, at : at + span]
        at += span
        near_down.append((piece, shifted(piece, 1), shifted(piece, -1)))

    outgoing, pick = dispatched(
        rank, expert_input, gain_expert[None, :], expert_choice.T, own_tokens, capacity, experts_all
    )
    arrived = exchanged(outgoing, experts_all)

    normed = rms_scale(mixer_input, gain_mixer)
    queries = jnp.dot(normed, query_weight, preferred_element_type=jnp.float32).astype(jnp.bfloat16)
    key_rows = jnp.dot(normed, key_weight, preferred_element_type=jnp.float32).astype(jnp.bfloat16)
    value_rows = jnp.dot(normed, value_weight, preferred_element_type=jnp.float32).astype(
        jnp.bfloat16
    )
    first_position = lax.axis_index("ep") % (ep_count // SEQS) * group_rows
    positions = (first_position + jnp.arange(group_rows, dtype=jnp.int32)).astype(jnp.float32)
    angles = positions[:, None] * frequencies(HEAD_DIM)[None, :]
    rot_queries = rotate(queries.reshape(group_rows, -1, HEAD_DIM), angles)
    rot_keys = rotate(key_rows.reshape(group_rows, -1, HEAD_DIM), angles)
    key_width = key_rows.shape[1]
    tail_start = group_rows - WINDOW
    tail_pair = jnp.concatenate(
        [rot_keys.reshape(group_rows, key_width)[tail_start:], value_rows[tail_start:]], axis=1
    )
    earlier_pair = from_behind(tail_pair, "ep", 1)
    normed_rows = rms_scale(expert_input, gain_expert)
    gate_values = jnp.dot(normed_rows, shared_gate, preferred_element_type=jnp.float32)
    up_values = jnp.dot(normed_rows, shared_up, preferred_element_type=jnp.float32)
    hidden = (jax.nn.silu(gate_values) * up_values).astype(jnp.bfloat16)
    shared_parts = halved_products(hidden, shared_down, own_tokens, 3)
    arrived, shared_parts = lax.optimization_barrier((arrived, shared_parts))
    near = expert_hidden(arrived, [(gate, up), (gate_left, up_left), (gate_right, up_right)])
    far = expert_hidden(arrived, [(gate_far, up_far)])
    returned = []
    for number, (piece, left, right) in enumerate(near_down):
        if number > 0:
            left, right, earlier_pair, _ = lax.optimization_barrier(
                (left, right, earlier_pair, result)
            )
        middle = left.shape[1] // 2
        far_left = shifted(left[:, :middle], 1)
        far_right = shifted(right[:, middle:], -1)
        result = expert_result(near, far, (piece, left, right, far_left, far_right))
        returned.append(exchanged(result, experts_all))

    prior_keys = earlier_pair[:, :key_width].reshape(WINDOW, -1, HEAD_DIM)
    prior_values = earlier_pair[:, key_width:].reshape(WINDOW, -1, HEAD_DIM)
    attended = attend(
        rot_queries,
        rot_keys,
        value_rows.reshape(group_rows, -1, HEAD_DIM),
        prior_keys,
        prior_values,
        first_position,
        sink_logits,
    )
    mixer_parts = halved_products(attended, output_weight, own_tokens, 1)
    mixer_output = halved_sum(*mixer_parts, 1).astype(jnp.bfloat16)
    shared_part = halved_sum(*shared_parts, 3)

    own_weights = lax.dynamic_slice_in_dim(route_weights, tp_rank * own_tokens, own_tokens, 0)
    mixing = jnp.sum(pick.astype(jnp.float32) * own_weights.T[:, None, :], axis=0)
    mixing = mixing.astype(jnp.bfloat16)
    done = []
    at = 0
    for part in returned:
        span = part.shape[1]
        routed = lax.dot_general(
            mixing, part, (((0,), (0,)), ((), ())), preferred_element_type=jnp.float32
        )
        done.append((routed + shared_part[:, at : at + span]).astype(jnp.bfloat16))
        at += span
    expert_output = jnp.concatenate(done, axis=1)
    return (mixer_output, expert_output)


def solution(mesh):
    placed = (
        P("ep", None),
        P("ep", None),
        P(),
        P(),
        P(None, "tp"),
        P(None, "tp"),
        P(None, "tp"),
        P("tp"),
        P("tp", None),
        P("ep", None),
        P("ep", None),
        P("ep", None, "tp"),
        P("ep", None, "tp"),
        P("ep", "tp", None),
        P(None, "tp"),
        P(None, "tp"),
        P("tp", None),
    )
    return jax.shard_map(
        both,
        mesh=mesh,
        in_specs=placed,
        out_specs=(P(("ep", "tp"), None), P(("ep", "tp"), None)),
        check_vma=False,
    )
```

```python
import math

import jax
import jax.numpy as jnp
from jax import lax
from jax.experimental import pallas as pl
from jax.experimental.pallas import tpu as pltpu
from jax.sharding import PartitionSpec as P


HEAD_DIM = 64
WINDOW = 128
SEQS = 1
SPANS = (768, 1280)


norm_eps = 1e-06
rope_base = 500000.0


def from_behind(value, axis, steps):
    count = lax.axis_size(axis)
    first, last = (max(0, -steps), min(count, count - steps))
    return lax.ppermute(value, axis, [(source, source + steps) for source in range(first, last)])


def shifted(value, steps):
    count = lax.axis_size("tp")
    return lax.ppermute(value, "tp", [(at, (at + steps) % count) for at in range(count)])


def crossed(value, mask):
    return lax.ppermute(value, "tp", [(at, at ^ mask) for at in range(lax.axis_size("tp"))])


def exchanged(rows, experts):
    slots, width = rows.shape
    return lax.all_to_all(
        rows.reshape(experts, slots // experts, width),
        "ep",
        split_axis=0,
        concat_axis=0,
        tiled=True,
    ).reshape(slots, width)


def halved_products(rows, weight, own_rows, mask):
    rank = lax.axis_index("tp")

    def product(*masks):
        blocks = [
            lax.dynamic_slice_in_dim(rows, (rank ^ each) * own_rows, own_rows, 0) for each in masks
        ]
        joined = jnp.concatenate(blocks, axis=0)
        return jnp.dot(joined, weight, preferred_element_type=jnp.float32).astype(jnp.bfloat16)

    return product(mask, 2), product(0, mask ^ 2)


def halved_sum(sent, kept, mask):
    own_rows = kept.shape[0] // 2
    got = crossed(sent, mask)
    half = kept.astype(jnp.float32) + got.astype(jnp.float32)
    last = crossed(half[own_rows:].astype(jnp.bfloat16), mask ^ 2)
    return half[:own_rows] + last.astype(jnp.float32)


def rms_scale(matrix, scaling):
    widened = matrix.astype(jnp.float32)
    scaled = widened * lax.rsqrt(jnp.mean(widened * widened, axis=-1, keepdims=True) + norm_eps)
    return (scaled * scaling).astype(jnp.bfloat16)


def frequencies(head_size):
    half_steps = jnp.arange(head_size // 2, dtype=jnp.float32)
    return rope_base ** (-(2.0 * half_steps) / head_size)


def rotate(heads, angles):
    middle = heads.shape[-1] // 2
    widened = heads.astype(jnp.float32)
    cosine = jnp.cos(angles)[:, None, :]
    sine_val = jnp.sin(angles)[:, None, :]
    leading = widened[..., :middle]
    trailing = widened[..., middle:]
    turned = jnp.concatenate(
        [leading * cosine - trailing * sine_val, trailing * cosine + leading * sine_val], axis=-1
    )
    return turned.astype(jnp.bfloat16)


def attend(
    query_heads, key_heads, value_heads, prior_keys, prior_values, first_position, sink_logits
):
    window = prior_keys.shape[0]
    total_rows, kv_count, head_size = key_heads.shape
    group_size = query_heads.shape[1] // kv_count
    blocks = total_rows // window

    def banded(earlier, current):
        joined = jnp.concatenate([earlier, current], axis=0).reshape(
            blocks + 1, window, kv_count, head_size
        )
        return jnp.concatenate([joined[:-1], joined[1:]], axis=1)

    band_keys = banded(prior_keys, key_heads)
    band_values = banded(prior_values, value_heads)
    query_blocks = query_heads.reshape(blocks, window, kv_count, group_size, head_size)
    scores = jnp.einsum(
        "nqhgd,nkhd->nhgqk", query_blocks, band_keys, preferred_element_type=jnp.float32
    ) / math.sqrt(head_size)
    query_index = jnp.arange(window, dtype=jnp.int32)[:, None]
    key_index = jnp.arange(2 * window, dtype=jnp.int32)[None, :]
    distance = query_index + window - key_index
    block_start = first_position + jnp.arange(blocks, dtype=jnp.int32)[:, None, None] * window
    allowed = (distance >= 0) & (distance < window) & (block_start - window + key_index >= 0)
    scores = jnp.where(allowed[:, None, None, :, :], scores, -jnp.inf)
    sink_grid = sink_logits.reshape(kv_count, group_size)[None, :, :, None, None]
    row_peak = jnp.maximum(jnp.max(scores, axis=-1, keepdims=True), sink_grid)
    shifted_exp = jnp.exp(scores - row_peak)
    denominator = jnp.sum(shifted_exp, axis=-1, keepdims=True) + jnp.exp(sink_grid - row_peak)
    probs = (shifted_exp / denominator).astype(jnp.bfloat16)
    attended = jnp.einsum(
        "nhgqk,nkhd->nqhgd", probs, band_values, preferred_element_type=jnp.float32
    )
    return attended.astype(jnp.bfloat16).reshape(total_rows, kv_count * group_size * head_size)


def dispatch_kernel(capacity, experts):
    def body(rank_ref, rows_ref, gain_ref, choice_ref, out_ref, pick_ref):
        rows = rows_ref[...].astype(jnp.float32)
        tokens = rows.shape[0]
        slots = experts * capacity
        scale = lax.rsqrt(jnp.mean(rows * rows, axis=-1, keepdims=True) + norm_eps)
        normed = (rows * scale * gain_ref[...]).astype(jnp.bfloat16)
        first = choice_ref[0:1, :]
        second = choice_ref[1:2, :]
        expert = lax.broadcasted_iota(jnp.int32, (experts, tokens), 0)
        named = jnp.where((first == expert) | (second == expert), 1.0, 0.0).astype(jnp.bfloat16)
        row = lax.broadcasted_iota(jnp.int32, (tokens, tokens), 0)
        col = lax.broadcasted_iota(jnp.int32, (tokens, tokens), 1)
        earlier = jnp.where(row < col, 1.0, 0.0).astype(jnp.bfloat16)
        ranks = jnp.dot(named, earlier, preferred_element_type=jnp.float32)
        slot_rank = jnp.broadcast_to(
            ranks.astype(jnp.int32)[:, None, :], (experts, capacity, tokens)
        ).reshape(slots, tokens)
        slot = lax.broadcasted_iota(jnp.int32, (slots, tokens), 0)
        fits = slot_rank == slot % capacity
        owner = slot // capacity
        pick_first = jnp.where((owner == first) & fits, 1.0, 0.0).astype(jnp.bfloat16)
        pick_second = jnp.where((owner == second) & fits, 1.0, 0.0).astype(jnp.bfloat16)
        pick_ref[0] = pick_first
        pick_ref[1] = pick_second
        out_ref[...] = jnp.dot(
            pick_first + pick_second, normed, preferred_element_type=jnp.float32
        ).astype(jnp.bfloat16)

    return body


def dispatched(rank, rows, gain, choice, tokens, capacity, experts):
    width = rows.shape[1]
    slots = experts * capacity
    return pl.pallas_call(
        dispatch_kernel(capacity, experts),
        grid_spec=pltpu.PrefetchScalarGridSpec(
            num_scalar_prefetch=1,
            grid=(1,),
            in_specs=[
                pl.BlockSpec((tokens, width), lambda i, r: (r[0], 0)),
                pl.BlockSpec((1, width), lambda i, r: (0, 0)),
                pl.BlockSpec((2, tokens), lambda i, r: (0, r[0])),
            ],
            out_specs=[
                pl.BlockSpec((slots, width), lambda i, r: (0, 0)),
                pl.BlockSpec((2, slots, tokens), lambda i, r: (0, 0, 0)),
            ],
        ),
        out_shape=[
            jax.ShapeDtypeStruct((slots, width), jnp.bfloat16),
            jax.ShapeDtypeStruct((2, slots, tokens), jnp.bfloat16),
        ],
        name="dispatch",
    )(rank, rows, gain, choice)


def hidden_body(rows_ref, *refs):
    count = len(refs) - 4
    sources, (out_ref, rows, held, sems) = refs[:count], refs[count:]
    units = held.shape[2] // 2
    copies = [pltpu.make_async_copy(rows_ref, rows, sems.at[count])]
    for at, source in enumerate(sources):
        place = held.at[at // 2, :, pl.ds(at % 2 * units, units)]
        copies.append(pltpu.make_async_copy(source, place, sems.at[at]))
    for copy in copies:
        copy.start()
    copies[0].wait()
    for index in range(held.shape[0]):
        copies[1 + 2 * index].wait()
        copies[2 + 2 * index].wait()
        both_values = jnp.dot(rows[...], held[index], preferred_element_type=jnp.float32)
        gate = both_values[:, :units]
        up = both_values[:, units:]
        out_ref[:, index * units : (index + 1) * units] = (
            gate / (1.0 + jnp.exp(-gate)) * up
        ).astype(jnp.bfloat16)


def expert_hidden(rows, pairs):
    slots, width = rows.shape
    units = pairs[0][0].shape[1]
    flat = [matrix for pair in pairs for matrix in pair]
    return pl.pallas_call(
        hidden_body,
        grid=(1,),
        in_specs=[pl.BlockSpec(memory_space=pl.ANY)] * (1 + len(flat)),
        out_specs=pl.BlockSpec((slots, len(pairs) * units), lambda i: (0, 0)),
        out_shape=jax.ShapeDtypeStruct((slots, len(pairs) * units), jnp.bfloat16),
        scratch_shapes=[
            pltpu.VMEM((slots, width), rows.dtype),
            pltpu.VMEM((len(pairs), width, 2 * units), rows.dtype),
            pltpu.SemaphoreType.DMA((len(flat) + 1,)),
        ],
    )(rows, *flat)


def down_kernel(counts):
    def body(near_ref, far_ref, *refs):
        out_ref = refs[-1]
        units = refs[0].shape[0]
        halves = max(counts)
        span = out_ref.shape[1] // halves
        for half in range(halves):
            total = 0.0
            first = 0
            for index, count in enumerate(counts):
                if index < 3:
                    hidden = near_ref[:, index * units : (index + 1) * units]
                else:
                    hidden = far_ref[...]
                if count == halves:
                    piece = refs[first + half][...]
                else:
                    piece = refs[first][:, half * span : (half + 1) * span]
                total = total + jnp.dot(hidden, piece, preferred_element_type=jnp.float32)
                first += count
            out_ref[:, half * span : (half + 1) * span] = total.astype(jnp.bfloat16)

    return body


def expert_result(near, far, matrices, steps=2):
    slots = near.shape[0]
    block = slots // steps
    width = sum(piece.shape[1] for piece in matrices[0])
    flat = [piece for pieces in matrices for piece in pieces]
    by_rows = lambda columns: pl.BlockSpec((block, columns), lambda i: (i, 0))
    return pl.pallas_call(
        down_kernel([len(pieces) for pieces in matrices]),
        grid=(steps,),
        in_specs=[by_rows(near.shape[1]), by_rows(far.shape[1])]
        + [pl.BlockSpec(piece.shape, lambda i: (0, 0)) for piece in flat],
        out_specs=by_rows(width),
        out_shape=jax.ShapeDtypeStruct((slots, width), jnp.bfloat16),
        name="down",
    )(near, far, *flat)


def both(
    mixer_input,
    expert_input,
    gain_mixer,
    gain_expert,
    query_weight,
    key_weight,
    value_weight,
    sink_logits,
    output_weight,
    expert_choice,
    route_weights,
    expert_gate,
    expert_up,
    expert_down,
    shared_gate,
    shared_up,
    shared_down,
):
    tp_count = lax.axis_size("tp")
    ep_count = lax.axis_size("ep")
    tp_rank = lax.axis_index("tp")
    rank = tp_rank.astype(jnp.int32).reshape(1)
    group_rows, _ = mixer_input.shape
    group_tokens = expert_input.shape[0]
    own_tokens = group_tokens // tp_count
    top_count = expert_choice.shape[1]
    experts_all = ep_count
    capacity = 2 * own_tokens * top_count // experts_all

    gate, up, down = expert_gate[0], expert_up[0], expert_down[0]
    gate_left, gate_right = shifted(gate, 1), shifted(gate, -1)
    up_left, up_right = shifted(up, 1), shifted(up, -1)
    gate_far, up_far = shifted(gate_left, 1), shifted(up_right, -1)
    first, second = SPANS
    half = first // 2
    piece = down[:, :first]
    left, right = shifted(piece, 1), shifted(piece, -1)
    far_pieces = (shifted(left[:, :half], 1), shifted(right[:, half:], -1))
    first_down = ((piece,), (left,), (right,), far_pieces)
    half = first + second // 2
    pieces = (down[:, first:half], down[:, half:])
    lefts = [shifted(piece, 1) for piece in pieces]
    rights = [shifted(piece, -1) for piece in pieces]
    far_pieces = (shifted(lefts[0], 1), shifted(rights[1], -1))
    second_down = (pieces, lefts, rights, far_pieces)

    outgoing, pick = dispatched(
        rank, expert_input, gain_expert[None, :], expert_choice.T, own_tokens, capacity, experts_all
    )
    arrived = exchanged(outgoing, experts_all)

    normed = rms_scale(mixer_input, gain_mixer)
    queries = jnp.dot(normed, query_weight, preferred_element_type=jnp.float32).astype(jnp.bfloat16)
    key_rows = jnp.dot(normed, key_weight, preferred_element_type=jnp.float32).astype(jnp.bfloat16)
    value_rows = jnp.dot(normed, value_weight, preferred_element_type=jnp.float32).astype(
        jnp.bfloat16
    )
    first_position = lax.axis_index("ep") % (ep_count // SEQS) * group_rows
    positions = (first_position + jnp.arange(group_rows, dtype=jnp.int32)).astype(jnp.float32)
    angles = positions[:, None] * frequencies(HEAD_DIM)[None, :]
    rot_queries = rotate(queries.reshape(group_rows, -1, HEAD_DIM), angles)
    rot_keys = rotate(key_rows.reshape(group_rows, -1, HEAD_DIM), angles)
    key_width = key_rows.shape[1]
    tail_start = group_rows - WINDOW
    tail_pair = jnp.concatenate(
        [rot_keys.reshape(group_rows, key_width)[tail_start:], value_rows[tail_start:]], axis=1
    )
    earlier_pair = from_behind(tail_pair, "ep", 1)
    normed_rows = rms_scale(expert_input, gain_expert)
    gate_values = jnp.dot(normed_rows, shared_gate, preferred_element_type=jnp.float32)
    up_values = jnp.dot(normed_rows, shared_up, preferred_element_type=jnp.float32)
    hidden = (jax.nn.silu(gate_values) * up_values).astype(jnp.bfloat16)
    shared_parts = halved_products(hidden, shared_down, own_tokens, 3)
    arrived, shared_parts = lax.optimization_barrier((arrived, shared_parts))
    near = expert_hidden(arrived, [(gate, up), (gate_left, up_left), (gate_right, up_right)])
    far = expert_hidden(arrived, [(gate_far, up_far)])
    own_weights = lax.dynamic_slice_in_dim(route_weights, tp_rank * own_tokens, own_tokens, 0)
    mixing = jnp.sum(pick.astype(jnp.float32) * own_weights.T[:, None, :], axis=0)
    mixing = mixing.astype(jnp.bfloat16)

    def weighted(part):
        return lax.dot_general(
            mixing, part, (((0,), (0,)), ((), ())), preferred_element_type=jnp.float32
        )

    result = expert_result(near, far, first_down)
    earlier_pair, _ = lax.optimization_barrier((earlier_pair, result))
    returned = [exchanged(result, experts_all)]
    result = expert_result(near, far, second_down)
    routed = [weighted(returned[0])]
    result, routed[0] = lax.optimization_barrier((result, routed[0]))
    returned.append(exchanged(result, experts_all))

    prior_keys = earlier_pair[:, :key_width].reshape(WINDOW, -1, HEAD_DIM)
    prior_values = earlier_pair[:, key_width:].reshape(WINDOW, -1, HEAD_DIM)
    attended = attend(
        rot_queries,
        rot_keys,
        value_rows.reshape(group_rows, -1, HEAD_DIM),
        prior_keys,
        prior_values,
        first_position,
        sink_logits,
    )
    mixer_parts = halved_products(attended, output_weight, own_tokens, 1)
    mixer_output = halved_sum(*mixer_parts, 1).astype(jnp.bfloat16)

    routed.append(weighted(returned[1]))
    shared_part = halved_sum(*shared_parts, 3)
    first = routed[0].shape[1]
    expert_output = jnp.concatenate(
        [
            (routed[0] + shared_part[:, :first]).astype(jnp.bfloat16),
            (routed[1] + shared_part[:, first:]).astype(jnp.bfloat16),
        ],
        axis=1,
    )
    return (mixer_output, expert_output)


def solution(mesh):
    placed = (
        P("ep", None),
        P("ep", None),
        P(),
        P(),
        P(None, "tp"),
        P(None, "tp"),
        P(None, "tp"),
        P("tp"),
        P("tp", None),
        P("ep", None),
        P("ep", None),
        P("ep", None, "tp"),
        P("ep", None, "tp"),
        P("ep", "tp", None),
        P(None, "tp"),
        P(None, "tp"),
        P("tp", None),
    )
    return jax.shard_map(
        both,
        mesh=mesh,
        in_specs=placed,
        out_specs=(P(("ep", "tp"), None), P(("ep", "tp"), None)),
        check_vma=False,
    )
```

```python
import math

import jax
import jax.numpy as jnp
from jax import lax
from jax.experimental import pallas as pl
from jax.experimental.pallas import tpu as pltpu
from jax.sharding import PartitionSpec as P


HEAD_DIM = 64
WINDOW = 128
SEQS = 1
SPANS = (768, 1280)


norm_eps = 1e-06
rope_base = 500000.0


def from_behind(value, axis, steps):
    count = lax.axis_size(axis)
    first, last = (max(0, -steps), min(count, count - steps))
    return lax.ppermute(value, axis, [(source, source + steps) for source in range(first, last)])


def shifted(value, steps):
    count = lax.axis_size("tp")
    return lax.ppermute(value, "tp", [(at, (at + steps) % count) for at in range(count)])


def crossed(value, mask):
    return lax.ppermute(value, "tp", [(at, at ^ mask) for at in range(lax.axis_size("tp"))])


def exchanged(rows, experts):
    slots, width = rows.shape
    return lax.all_to_all(
        rows.reshape(experts, slots // experts, width),
        "ep",
        split_axis=0,
        concat_axis=0,
        tiled=True,
    ).reshape(slots, width)


def halved_products(rows, weight, own_rows, mask):
    rank = lax.axis_index("tp")

    def product(*masks):
        blocks = [
            lax.dynamic_slice_in_dim(rows, (rank ^ each) * own_rows, own_rows, 0) for each in masks
        ]
        joined = jnp.concatenate(blocks, axis=0)
        return jnp.dot(joined, weight, preferred_element_type=jnp.float32).astype(jnp.bfloat16)

    return product(mask, 2), product(0, mask ^ 2)


def halved_sum(sent, kept, mask):
    own_rows = kept.shape[0] // 2
    got = crossed(sent, mask)
    half = kept.astype(jnp.float32) + got.astype(jnp.float32)
    last = crossed(half[own_rows:].astype(jnp.bfloat16), mask ^ 2)
    return half[:own_rows] + last.astype(jnp.float32)


def rms_scale(matrix, scaling):
    widened = matrix.astype(jnp.float32)
    scaled = widened * lax.rsqrt(jnp.mean(widened * widened, axis=-1, keepdims=True) + norm_eps)
    return (scaled * scaling).astype(jnp.bfloat16)


def frequencies(head_size):
    half_steps = jnp.arange(head_size // 2, dtype=jnp.float32)
    return rope_base ** (-(2.0 * half_steps) / head_size)


def rotate(heads, angles):
    middle = heads.shape[-1] // 2
    widened = heads.astype(jnp.float32)
    cosine = jnp.cos(angles)[:, None, :]
    sine_val = jnp.sin(angles)[:, None, :]
    leading = widened[..., :middle]
    trailing = widened[..., middle:]
    turned = jnp.concatenate(
        [leading * cosine - trailing * sine_val, trailing * cosine + leading * sine_val], axis=-1
    )
    return turned.astype(jnp.bfloat16)


def attend(
    query_heads, key_heads, value_heads, prior_keys, prior_values, first_position, sink_logits
):
    window = prior_keys.shape[0]
    total_rows, kv_count, head_size = key_heads.shape
    group_size = query_heads.shape[1] // kv_count
    blocks = total_rows // window

    def banded(earlier, current):
        joined = jnp.concatenate([earlier, current], axis=0).reshape(
            blocks + 1, window, kv_count, head_size
        )
        return jnp.concatenate([joined[:-1], joined[1:]], axis=1)

    band_keys = banded(prior_keys, key_heads)
    band_values = banded(prior_values, value_heads)
    query_blocks = query_heads.reshape(blocks, window, kv_count, group_size, head_size)
    scores = jnp.einsum(
        "nqhgd,nkhd->nhgqk", query_blocks, band_keys, preferred_element_type=jnp.float32
    ) / math.sqrt(head_size)
    query_index = jnp.arange(window, dtype=jnp.int32)[:, None]
    key_index = jnp.arange(2 * window, dtype=jnp.int32)[None, :]
    distance = query_index + window - key_index
    block_start = first_position + jnp.arange(blocks, dtype=jnp.int32)[:, None, None] * window
    allowed = (distance >= 0) & (distance < window) & (block_start - window + key_index >= 0)
    scores = jnp.where(allowed[:, None, None, :, :], scores, -jnp.inf)
    sink_grid = sink_logits.reshape(kv_count, group_size)[None, :, :, None, None]
    row_peak = jnp.maximum(jnp.max(scores, axis=-1, keepdims=True), sink_grid)
    shifted_exp = jnp.exp(scores - row_peak)
    denominator = jnp.sum(shifted_exp, axis=-1, keepdims=True) + jnp.exp(sink_grid - row_peak)
    probs = (shifted_exp / denominator).astype(jnp.bfloat16)
    attended = jnp.einsum(
        "nhgqk,nkhd->nqhgd", probs, band_values, preferred_element_type=jnp.float32
    )
    return attended.astype(jnp.bfloat16).reshape(total_rows, kv_count * group_size * head_size)


def dispatch_kernel(capacity, experts):
    def body(rank_ref, rows_ref, gain_ref, choice_ref, out_ref, pick_ref):
        rows = rows_ref[...].astype(jnp.float32)
        tokens = rows.shape[0]
        slots = experts * capacity
        scale = lax.rsqrt(jnp.mean(rows * rows, axis=-1, keepdims=True) + norm_eps)
        normed = (rows * scale * gain_ref[...]).astype(jnp.bfloat16)
        first = choice_ref[0:1, :]
        second = choice_ref[1:2, :]
        expert = lax.broadcasted_iota(jnp.int32, (experts, tokens), 0)
        named = jnp.where((first == expert) | (second == expert), 1.0, 0.0).astype(jnp.bfloat16)
        row = lax.broadcasted_iota(jnp.int32, (tokens, tokens), 0)
        col = lax.broadcasted_iota(jnp.int32, (tokens, tokens), 1)
        earlier = jnp.where(row < col, 1.0, 0.0).astype(jnp.bfloat16)
        ranks = jnp.dot(named, earlier, preferred_element_type=jnp.float32)
        slot_rank = jnp.broadcast_to(
            ranks.astype(jnp.int32)[:, None, :], (experts, capacity, tokens)
        ).reshape(slots, tokens)
        slot = lax.broadcasted_iota(jnp.int32, (slots, tokens), 0)
        fits = slot_rank == slot % capacity
        owner = slot // capacity
        pick_first = jnp.where((owner == first) & fits, 1.0, 0.0).astype(jnp.bfloat16)
        pick_second = jnp.where((owner == second) & fits, 1.0, 0.0).astype(jnp.bfloat16)
        pick_ref[0] = pick_first
        pick_ref[1] = pick_second
        out_ref[...] = jnp.dot(
            pick_first + pick_second, normed, preferred_element_type=jnp.float32
        ).astype(jnp.bfloat16)

    return body


def dispatched(rank, rows, gain, choice, tokens, capacity, experts):
    width = rows.shape[1]
    slots = experts * capacity
    return pl.pallas_call(
        dispatch_kernel(capacity, experts),
        grid_spec=pltpu.PrefetchScalarGridSpec(
            num_scalar_prefetch=1,
            grid=(1,),
            in_specs=[
                pl.BlockSpec((tokens, width), lambda i, r: (r[0], 0)),
                pl.BlockSpec((1, width), lambda i, r: (0, 0)),
                pl.BlockSpec((2, tokens), lambda i, r: (0, r[0])),
            ],
            out_specs=[
                pl.BlockSpec((slots, width), lambda i, r: (0, 0)),
                pl.BlockSpec((2, slots, tokens), lambda i, r: (0, 0, 0)),
            ],
        ),
        out_shape=[
            jax.ShapeDtypeStruct((slots, width), jnp.bfloat16),
            jax.ShapeDtypeStruct((2, slots, tokens), jnp.bfloat16),
        ],
        name="dispatch",
    )(rank, rows, gain, choice)


def hidden_body(rows_ref, *refs):
    count = len(refs) - 4
    sources, (out_ref, rows, held, sems) = refs[:count], refs[count:]
    units = held.shape[2] // 2
    copies = [pltpu.make_async_copy(rows_ref, rows, sems.at[count])]
    for at, source in enumerate(sources):
        place = held.at[at // 2, :, pl.ds(at % 2 * units, units)]
        copies.append(pltpu.make_async_copy(source, place, sems.at[at]))
    for copy in copies:
        copy.start()
    copies[0].wait()
    for index in range(held.shape[0]):
        copies[1 + 2 * index].wait()
        copies[2 + 2 * index].wait()
        both_values = jnp.dot(rows[...], held[index], preferred_element_type=jnp.float32)
        gate = both_values[:, :units]
        up = both_values[:, units:]
        out_ref[:, index * units : (index + 1) * units] = (
            gate / (1.0 + jnp.exp(-gate)) * up
        ).astype(jnp.bfloat16)


def expert_hidden(rows, pairs):
    slots, width = rows.shape
    units = pairs[0][0].shape[1]
    flat = [matrix for pair in pairs for matrix in pair]
    return pl.pallas_call(
        hidden_body,
        grid=(1,),
        in_specs=[pl.BlockSpec(memory_space=pl.ANY)] * (1 + len(flat)),
        out_specs=pl.BlockSpec((slots, len(pairs) * units), lambda i: (0, 0)),
        out_shape=jax.ShapeDtypeStruct((slots, len(pairs) * units), jnp.bfloat16),
        scratch_shapes=[
            pltpu.VMEM((slots, width), rows.dtype),
            pltpu.VMEM((len(pairs), width, 2 * units), rows.dtype),
            pltpu.SemaphoreType.DMA((len(flat) + 1,)),
        ],
    )(rows, *flat)


def down_kernel(counts):
    def body(near_ref, far_ref, *refs):
        out_ref = refs[-1]
        units = refs[0].shape[0]
        halves = max(counts)
        span = out_ref.shape[1] // halves
        for half in range(halves):
            total = 0.0
            first = 0
            for index, count in enumerate(counts):
                if index < 3:
                    hidden = near_ref[:, index * units : (index + 1) * units]
                else:
                    hidden = far_ref[...]
                if count == halves:
                    piece = refs[first + half][...]
                else:
                    piece = refs[first][:, half * span : (half + 1) * span]
                total = total + jnp.dot(hidden, piece, preferred_element_type=jnp.float32)
                first += count
            out_ref[:, half * span : (half + 1) * span] = total.astype(jnp.bfloat16)

    return body


def expert_result(near, far, matrices, steps=2):
    slots = near.shape[0]
    block = slots // steps
    width = sum(piece.shape[1] for piece in matrices[0])
    flat = [piece for pieces in matrices for piece in pieces]
    by_rows = lambda columns: pl.BlockSpec((block, columns), lambda i: (i, 0))
    return pl.pallas_call(
        down_kernel([len(pieces) for pieces in matrices]),
        grid=(steps,),
        in_specs=[by_rows(near.shape[1]), by_rows(far.shape[1])]
        + [pl.BlockSpec(piece.shape, lambda i: (0, 0)) for piece in flat],
        out_specs=by_rows(width),
        out_shape=jax.ShapeDtypeStruct((slots, width), jnp.bfloat16),
        name="down",
    )(near, far, *flat)


def both(
    mixer_input,
    expert_input,
    gain_mixer,
    gain_expert,
    query_weight,
    key_weight,
    value_weight,
    sink_logits,
    output_weight,
    expert_choice,
    route_weights,
    expert_gate,
    expert_up,
    expert_down,
    shared_gate,
    shared_up,
    shared_down,
):
    tp_count = lax.axis_size("tp")
    ep_count = lax.axis_size("ep")
    tp_rank = lax.axis_index("tp")
    rank = tp_rank.astype(jnp.int32).reshape(1)
    group_rows, model_width = mixer_input.shape
    group_tokens = expert_input.shape[0]
    own_tokens = group_tokens // tp_count
    top_count = expert_choice.shape[1]
    experts_all = ep_count
    capacity = 2 * own_tokens * top_count // experts_all

    gate, up, down = expert_gate[0], expert_up[0], expert_down[0]
    gate_left, gate_right = shifted(gate, 1), shifted(gate, -1)
    up_left, up_right = shifted(up, 1), shifted(up, -1)
    gate_far, up_far = shifted(gate_left, 1), shifted(up_right, -1)
    first, second = SPANS
    half = first // 2
    piece = down[:, :first]
    left, right = shifted(piece, 1), shifted(piece, -1)
    far_pieces = (shifted(left[:, :half], 1), shifted(right[:, half:], -1))
    first_down = ((piece,), (left,), (right,), far_pieces)
    half = first + second // 2
    pieces = (down[:, first:half], down[:, half:])
    lefts = [shifted(piece, 1) for piece in pieces]
    rights = [shifted(piece, -1) for piece in pieces]
    far_pieces = (shifted(lefts[0], 1), shifted(rights[1], -1))
    second_down = (pieces, lefts, rights, far_pieces)

    outgoing, pick = dispatched(
        rank, expert_input, gain_expert[None, :], expert_choice.T, own_tokens, capacity, experts_all
    )
    arrived = exchanged(outgoing, experts_all)

    normed = rms_scale(mixer_input, gain_mixer)
    queries = jnp.dot(normed, query_weight, preferred_element_type=jnp.float32).astype(jnp.bfloat16)
    key_rows = jnp.dot(normed, key_weight, preferred_element_type=jnp.float32).astype(jnp.bfloat16)
    value_rows = jnp.dot(normed, value_weight, preferred_element_type=jnp.float32).astype(
        jnp.bfloat16
    )
    first_position = lax.axis_index("ep") % (ep_count // SEQS) * group_rows
    positions = (first_position + jnp.arange(group_rows, dtype=jnp.int32)).astype(jnp.float32)
    angles = positions[:, None] * frequencies(HEAD_DIM)[None, :]
    rot_queries = rotate(queries.reshape(group_rows, -1, HEAD_DIM), angles)
    rot_keys = rotate(key_rows.reshape(group_rows, -1, HEAD_DIM), angles)
    key_width = key_rows.shape[1]
    tail_start = group_rows - WINDOW
    tail_pair = jnp.concatenate(
        [rot_keys.reshape(group_rows, key_width)[tail_start:], value_rows[tail_start:]], axis=1
    )
    earlier_pair = from_behind(tail_pair, "ep", 1)
    normed_rows = rms_scale(expert_input, gain_expert)
    gate_values = jnp.dot(normed_rows, shared_gate, preferred_element_type=jnp.float32)
    up_values = jnp.dot(normed_rows, shared_up, preferred_element_type=jnp.float32)
    hidden = (jax.nn.silu(gate_values) * up_values).astype(jnp.bfloat16)
    shared_parts = halved_products(hidden, shared_down, own_tokens, 3)
    arrived, shared_parts = lax.optimization_barrier((arrived, shared_parts))
    near = expert_hidden(arrived, [(gate, up), (gate_left, up_left), (gate_right, up_right)])
    far = expert_hidden(arrived, [(gate_far, up_far)])
    own_weights = lax.dynamic_slice_in_dim(route_weights, tp_rank * own_tokens, own_tokens, 0)
    mixing = jnp.sum(pick.astype(jnp.float32) * own_weights.T[:, None, :], axis=0)
    mixing = mixing.astype(jnp.bfloat16)

    def weighted(part):
        return lax.dot_general(
            mixing, part, (((0,), (0,)), ((), ())), preferred_element_type=jnp.float32
        )

    result = expert_result(near, far, first_down)
    earlier_pair, _ = lax.optimization_barrier((earlier_pair, result))
    returned = [exchanged(result, experts_all)]
    result = expert_result(near, far, second_down)
    routed = [weighted(returned[0])]
    result, routed[0] = lax.optimization_barrier((result, routed[0]))
    returned.append(exchanged(result, experts_all))

    prior_keys = earlier_pair[:, :key_width].reshape(WINDOW, -1, HEAD_DIM)
    prior_values = earlier_pair[:, key_width:].reshape(WINDOW, -1, HEAD_DIM)
    attended = attend(
        rot_queries,
        rot_keys,
        value_rows.reshape(group_rows, -1, HEAD_DIM),
        prior_keys,
        prior_values,
        first_position,
        sink_logits,
    )
    mixer_parts = halved_products(attended, output_weight, own_tokens, 1)
    mixer_output = halved_sum(*mixer_parts, 1).astype(jnp.bfloat16)

    routed.append(weighted(returned[1]))
    shared_part = halved_sum(*shared_parts, 3)
    first = routed[0].shape[1]
    head = (routed[0] + shared_part[:, :first]).astype(jnp.bfloat16)
    head = lax.optimization_barrier(jnp.pad(head, ((0, 0), (0, model_width - first))))
    tail = (routed[1] + shared_part[:, first:]).astype(jnp.bfloat16)
    expert_output = lax.dynamic_update_slice(head, tail, (0, first))
    return (mixer_output, expert_output)


def solution(mesh):
    placed = (
        P("ep", None),
        P("ep", None),
        P(),
        P(),
        P(None, "tp"),
        P(None, "tp"),
        P(None, "tp"),
        P("tp"),
        P("tp", None),
        P("ep", None),
        P("ep", None),
        P("ep", None, "tp"),
        P("ep", None, "tp"),
        P("ep", "tp", None),
        P(None, "tp"),
        P(None, "tp"),
        P("tp", None),
    )
    return jax.shard_map(
        both,
        mesh=mesh,
        in_specs=placed,
        out_specs=(P(("ep", "tp"), None), P(("ep", "tp"), None)),
        check_vma=False,
    )
```

```python
import math

import jax
import jax.numpy as jnp
from jax import lax
from jax.experimental import pallas as pl
from jax.experimental.pallas import tpu as pltpu
from jax.sharding import PartitionSpec as P


HEAD_DIM = 64
WINDOW = 128
SEQS = 1
SPANS = (768, 1280)


norm_eps = 1e-06
rope_base = 500000.0


def from_behind(value, axis, steps):
    count = lax.axis_size(axis)
    first, last = (max(0, -steps), min(count, count - steps))
    return lax.ppermute(value, axis, [(source, source + steps) for source in range(first, last)])


def shifted(value, steps):
    count = lax.axis_size("tp")
    return lax.ppermute(value, "tp", [(at, (at + steps) % count) for at in range(count)])


def crossed(value, mask):
    return lax.ppermute(value, "tp", [(at, at ^ mask) for at in range(lax.axis_size("tp"))])


def exchanged(rows, experts):
    slots, width = rows.shape
    return lax.all_to_all(
        rows.reshape(experts, slots // experts, width),
        "ep",
        split_axis=0,
        concat_axis=0,
        tiled=True,
    ).reshape(slots, width)


def halved_products(rows, weight, own_rows, mask):
    rank = lax.axis_index("tp")

    def product(*masks):
        blocks = [
            lax.dynamic_slice_in_dim(rows, (rank ^ each) * own_rows, own_rows, 0) for each in masks
        ]
        joined = jnp.concatenate(blocks, axis=0)
        return jnp.dot(joined, weight, preferred_element_type=jnp.float32).astype(jnp.bfloat16)

    return product(mask, 2), product(0, mask ^ 2)


def halved_sum(sent, kept, mask):
    own_rows = kept.shape[0] // 2
    got = crossed(sent, mask)
    half = kept.astype(jnp.float32) + got.astype(jnp.float32)
    last = crossed(half[own_rows:].astype(jnp.bfloat16), mask ^ 2)
    return half[:own_rows] + last.astype(jnp.float32)


def rms_scale(matrix, scaling):
    widened = matrix.astype(jnp.float32)
    scaled = widened * lax.rsqrt(jnp.mean(widened * widened, axis=-1, keepdims=True) + norm_eps)
    return (scaled * scaling).astype(jnp.bfloat16)


def frequencies(head_size):
    half_steps = jnp.arange(head_size // 2, dtype=jnp.float32)
    return rope_base ** (-(2.0 * half_steps) / head_size)


def rotate(heads, angles):
    middle = heads.shape[-1] // 2
    widened = heads.astype(jnp.float32)
    cosine = jnp.cos(angles)[:, None, :]
    sine_val = jnp.sin(angles)[:, None, :]
    leading = widened[..., :middle]
    trailing = widened[..., middle:]
    turned = jnp.concatenate(
        [leading * cosine - trailing * sine_val, trailing * cosine + leading * sine_val], axis=-1
    )
    return turned.astype(jnp.bfloat16)


def attend(
    query_heads, key_heads, value_heads, prior_keys, prior_values, first_position, sink_logits
):
    window = prior_keys.shape[0]
    total_rows, kv_count, head_size = key_heads.shape
    group_size = query_heads.shape[1] // kv_count
    blocks = total_rows // window

    def banded(earlier, current):
        joined = jnp.concatenate([earlier, current], axis=0).reshape(
            blocks + 1, window, kv_count, head_size
        )
        return jnp.concatenate([joined[:-1], joined[1:]], axis=1)

    band_keys = banded(prior_keys, key_heads)
    band_values = banded(prior_values, value_heads)
    query_blocks = query_heads.reshape(blocks, window, kv_count, group_size, head_size)
    scores = jnp.einsum(
        "nqhgd,nkhd->nhgqk", query_blocks, band_keys, preferred_element_type=jnp.float32
    ) / math.sqrt(head_size)
    query_index = jnp.arange(window, dtype=jnp.int32)[:, None]
    key_index = jnp.arange(2 * window, dtype=jnp.int32)[None, :]
    distance = query_index + window - key_index
    block_start = first_position + jnp.arange(blocks, dtype=jnp.int32)[:, None, None] * window
    allowed = (distance >= 0) & (distance < window) & (block_start - window + key_index >= 0)
    scores = jnp.where(allowed[:, None, None, :, :], scores, -jnp.inf)
    sink_grid = sink_logits.reshape(kv_count, group_size)[None, :, :, None, None]
    row_peak = jnp.maximum(jnp.max(scores, axis=-1, keepdims=True), sink_grid)
    shifted_exp = jnp.exp(scores - row_peak)
    denominator = jnp.sum(shifted_exp, axis=-1, keepdims=True) + jnp.exp(sink_grid - row_peak)
    probs = (shifted_exp / denominator).astype(jnp.bfloat16)
    attended = jnp.einsum(
        "nhgqk,nkhd->nqhgd", probs, band_values, preferred_element_type=jnp.float32
    )
    return attended.astype(jnp.bfloat16).reshape(total_rows, kv_count * group_size * head_size)


def dispatch_kernel(capacity, experts):
    def body(rank_ref, rows_ref, gain_ref, choice_ref, out_ref, pick_ref):
        rows = rows_ref[...].astype(jnp.float32)
        tokens = rows.shape[0]
        slots = experts * capacity
        scale = lax.rsqrt(jnp.mean(rows * rows, axis=-1, keepdims=True) + norm_eps)
        normed = (rows * scale * gain_ref[...]).astype(jnp.bfloat16)
        first = choice_ref[0:1, :]
        second = choice_ref[1:2, :]
        expert = lax.broadcasted_iota(jnp.int32, (experts, tokens), 0)
        named = jnp.where((first == expert) | (second == expert), 1.0, 0.0).astype(jnp.bfloat16)
        row = lax.broadcasted_iota(jnp.int32, (tokens, tokens), 0)
        col = lax.broadcasted_iota(jnp.int32, (tokens, tokens), 1)
        earlier = jnp.where(row < col, 1.0, 0.0).astype(jnp.bfloat16)
        ranks = jnp.dot(named, earlier, preferred_element_type=jnp.float32)
        slot_rank = jnp.broadcast_to(
            ranks.astype(jnp.int32)[:, None, :], (experts, capacity, tokens)
        ).reshape(slots, tokens)
        slot = lax.broadcasted_iota(jnp.int32, (slots, tokens), 0)
        fits = slot_rank == slot % capacity
        owner = slot // capacity
        pick_first = jnp.where((owner == first) & fits, 1.0, 0.0).astype(jnp.bfloat16)
        pick_second = jnp.where((owner == second) & fits, 1.0, 0.0).astype(jnp.bfloat16)
        pick_ref[0] = pick_first
        pick_ref[1] = pick_second
        out_ref[...] = jnp.dot(
            pick_first + pick_second, normed, preferred_element_type=jnp.float32
        ).astype(jnp.bfloat16)

    return body


def dispatched(rank, rows, gain, choice, tokens, capacity, experts):
    width = rows.shape[1]
    slots = experts * capacity
    return pl.pallas_call(
        dispatch_kernel(capacity, experts),
        grid_spec=pltpu.PrefetchScalarGridSpec(
            num_scalar_prefetch=1,
            grid=(1,),
            in_specs=[
                pl.BlockSpec((tokens, width), lambda i, r: (r[0], 0)),
                pl.BlockSpec((1, width), lambda i, r: (0, 0)),
                pl.BlockSpec((2, tokens), lambda i, r: (0, r[0])),
            ],
            out_specs=[
                pl.BlockSpec((slots, width), lambda i, r: (0, 0)),
                pl.BlockSpec((2, slots, tokens), lambda i, r: (0, 0, 0)),
            ],
        ),
        out_shape=[
            jax.ShapeDtypeStruct((slots, width), jnp.bfloat16),
            jax.ShapeDtypeStruct((2, slots, tokens), jnp.bfloat16),
        ],
        name="dispatch",
    )(rank, rows, gain, choice)


def hidden_body(rows_ref, *refs):
    count = len(refs) - 4
    sources, (out_ref, rows, held, sems) = refs[:count], refs[count:]
    units = held.shape[2] // 2
    row_block = rows.shape[0] // (2 if held.shape[0] > 1 else 1)
    copies = [pltpu.make_async_copy(rows_ref, rows, sems.at[count])]
    for at, source in enumerate(sources):
        place = held.at[at // 2, :, pl.ds(at % 2 * units, units)]
        copies.append(pltpu.make_async_copy(source, place, sems.at[at]))
    for copy in copies:
        copy.start()
    copies[0].wait()
    for index in range(held.shape[0]):
        copies[1 + 2 * index].wait()
        copies[2 + 2 * index].wait()

        def block(step, carry, index=index):
            part = pl.ds(step * row_block, row_block)
            both_values = jnp.dot(rows[part, :], held[index], preferred_element_type=jnp.float32)
            gate = both_values[:, :units]
            up = both_values[:, units:]
            out_ref[part, index * units : (index + 1) * units] = (
                gate / (1.0 + jnp.exp(-gate)) * up
            ).astype(jnp.bfloat16)
            return carry

        lax.fori_loop(0, rows.shape[0] // row_block, block, 0)


def expert_hidden(rows, pairs):
    slots, width = rows.shape
    units = pairs[0][0].shape[1]
    flat = [matrix for pair in pairs for matrix in pair]
    return pl.pallas_call(
        hidden_body,
        grid=(1,),
        in_specs=[pl.BlockSpec(memory_space=pl.ANY)] * (1 + len(flat)),
        out_specs=pl.BlockSpec((slots, len(pairs) * units), lambda i: (0, 0)),
        out_shape=jax.ShapeDtypeStruct((slots, len(pairs) * units), jnp.bfloat16),
        scratch_shapes=[
            pltpu.VMEM((slots, width), rows.dtype),
            pltpu.VMEM((len(pairs), width, 2 * units), rows.dtype),
            pltpu.SemaphoreType.DMA((len(flat) + 1,)),
        ],
    )(rows, *flat)


def down_kernel(counts):
    def body(near_ref, far_ref, *refs):
        out_ref = refs[-1]
        units = refs[0].shape[0]
        halves = max(counts)
        span = out_ref.shape[1] // halves
        for half in range(halves):
            total = 0.0
            first = 0
            for index, count in enumerate(counts):
                if index < 3:
                    hidden = near_ref[:, index * units : (index + 1) * units]
                else:
                    hidden = far_ref[...]
                if count == halves:
                    piece = refs[first + half][...]
                else:
                    piece = refs[first][:, half * span : (half + 1) * span]
                total = total + jnp.dot(hidden, piece, preferred_element_type=jnp.float32)
                first += count
            out_ref[:, half * span : (half + 1) * span] = total.astype(jnp.bfloat16)

    return body


def expert_result(near, far, matrices, steps=2):
    slots = near.shape[0]
    block = slots // steps
    width = sum(piece.shape[1] for piece in matrices[0])
    flat = [piece for pieces in matrices for piece in pieces]
    by_rows = lambda columns: pl.BlockSpec((block, columns), lambda i: (i, 0))
    return pl.pallas_call(
        down_kernel([len(pieces) for pieces in matrices]),
        grid=(steps,),
        in_specs=[by_rows(near.shape[1]), by_rows(far.shape[1])]
        + [pl.BlockSpec(piece.shape, lambda i: (0, 0)) for piece in flat],
        out_specs=by_rows(width),
        out_shape=jax.ShapeDtypeStruct((slots, width), jnp.bfloat16),
        name="down",
    )(near, far, *flat)


def both(
    mixer_input,
    expert_input,
    gain_mixer,
    gain_expert,
    query_weight,
    key_weight,
    value_weight,
    sink_logits,
    output_weight,
    expert_choice,
    route_weights,
    expert_gate,
    expert_up,
    expert_down,
    shared_gate,
    shared_up,
    shared_down,
):
    tp_count = lax.axis_size("tp")
    ep_count = lax.axis_size("ep")
    tp_rank = lax.axis_index("tp")
    rank = tp_rank.astype(jnp.int32).reshape(1)
    group_rows, model_width = mixer_input.shape
    group_tokens = expert_input.shape[0]
    own_tokens = group_tokens // tp_count
    top_count = expert_choice.shape[1]
    experts_all = ep_count
    capacity = 2 * own_tokens * top_count // experts_all

    gate, up, down = expert_gate[0], expert_up[0], expert_down[0]
    gate_left, gate_right = shifted(gate, 1), shifted(gate, -1)
    up_left, up_right = shifted(up, 1), shifted(up, -1)
    gate_far, up_far = shifted(gate_left, 1), shifted(up_right, -1)
    first, second = SPANS
    half = first // 2
    piece = down[:, :first]
    left, right = shifted(piece, 1), shifted(piece, -1)
    far_pieces = (shifted(left[:, :half], 1), shifted(right[:, half:], -1))
    first_down = ((piece,), (left,), (right,), far_pieces)
    half = first + second // 2
    pieces = (down[:, first:half], down[:, half:])
    lefts = [shifted(piece, 1) for piece in pieces]
    rights = [shifted(piece, -1) for piece in pieces]
    far_pieces = (shifted(lefts[0], 1), shifted(rights[1], -1))
    second_down = (pieces, lefts, rights, far_pieces)

    outgoing, pick = dispatched(
        rank, expert_input, gain_expert[None, :], expert_choice.T, own_tokens, capacity, experts_all
    )
    arrived = exchanged(outgoing, experts_all)

    normed = rms_scale(mixer_input, gain_mixer)
    queries = jnp.dot(normed, query_weight, preferred_element_type=jnp.float32).astype(jnp.bfloat16)
    key_rows = jnp.dot(normed, key_weight, preferred_element_type=jnp.float32).astype(jnp.bfloat16)
    value_rows = jnp.dot(normed, value_weight, preferred_element_type=jnp.float32).astype(
        jnp.bfloat16
    )
    first_position = lax.axis_index("ep") % (ep_count // SEQS) * group_rows
    positions = (first_position + jnp.arange(group_rows, dtype=jnp.int32)).astype(jnp.float32)
    angles = positions[:, None] * frequencies(HEAD_DIM)[None, :]
    rot_queries = rotate(queries.reshape(group_rows, -1, HEAD_DIM), angles)
    rot_keys = rotate(key_rows.reshape(group_rows, -1, HEAD_DIM), angles)
    key_width = key_rows.shape[1]
    tail_start = group_rows - WINDOW
    tail_pair = jnp.concatenate(
        [rot_keys.reshape(group_rows, key_width)[tail_start:], value_rows[tail_start:]], axis=1
    )
    earlier_pair = from_behind(tail_pair, "ep", 1)
    normed_rows = rms_scale(expert_input, gain_expert)
    gate_values = jnp.dot(normed_rows, shared_gate, preferred_element_type=jnp.float32)
    up_values = jnp.dot(normed_rows, shared_up, preferred_element_type=jnp.float32)
    hidden = (jax.nn.silu(gate_values) * up_values).astype(jnp.bfloat16)
    shared_parts = halved_products(hidden, shared_down, own_tokens, 3)
    arrived, shared_parts = lax.optimization_barrier((arrived, shared_parts))
    near = expert_hidden(arrived, [(gate, up), (gate_left, up_left), (gate_right, up_right)])
    far = expert_hidden(arrived, [(gate_far, up_far)])
    own_weights = lax.dynamic_slice_in_dim(route_weights, tp_rank * own_tokens, own_tokens, 0)
    mixing = jnp.sum(pick.astype(jnp.float32) * own_weights.T[:, None, :], axis=0)
    mixing = mixing.astype(jnp.bfloat16)

    def weighted(part):
        return lax.dot_general(
            mixing, part, (((0,), (0,)), ((), ())), preferred_element_type=jnp.float32
        )

    result = expert_result(near, far, first_down)
    earlier_pair, _ = lax.optimization_barrier((earlier_pair, result))
    returned = [exchanged(result, experts_all)]
    result = expert_result(near, far, second_down)
    routed = [weighted(returned[0])]
    result, routed[0] = lax.optimization_barrier((result, routed[0]))
    returned.append(exchanged(result, experts_all))

    prior_keys = earlier_pair[:, :key_width].reshape(WINDOW, -1, HEAD_DIM)
    prior_values = earlier_pair[:, key_width:].reshape(WINDOW, -1, HEAD_DIM)
    attended = attend(
        rot_queries,
        rot_keys,
        value_rows.reshape(group_rows, -1, HEAD_DIM),
        prior_keys,
        prior_values,
        first_position,
        sink_logits,
    )
    mixer_parts = halved_products(attended, output_weight, own_tokens, 1)
    mixer_output = halved_sum(*mixer_parts, 1).astype(jnp.bfloat16)

    routed.append(weighted(returned[1]))
    shared_part = halved_sum(*shared_parts, 3)
    first = routed[0].shape[1]
    head = (routed[0] + shared_part[:, :first]).astype(jnp.bfloat16)
    head = lax.optimization_barrier(jnp.pad(head, ((0, 0), (0, model_width - first))))
    tail = (routed[1] + shared_part[:, first:]).astype(jnp.bfloat16)
    expert_output = lax.dynamic_update_slice(head, tail, (0, first))
    return (mixer_output, expert_output)


def solution(mesh):
    placed = (
        P("ep", None),
        P("ep", None),
        P(),
        P(),
        P(None, "tp"),
        P(None, "tp"),
        P(None, "tp"),
        P("tp"),
        P("tp", None),
        P("ep", None),
        P("ep", None),
        P("ep", None, "tp"),
        P("ep", None, "tp"),
        P("ep", "tp", None),
        P(None, "tp"),
        P(None, "tp"),
        P("tp", None),
    )
    return jax.shard_map(
        both,
        mesh=mesh,
        in_specs=placed,
        out_specs=(P(("ep", "tp"), None), P(("ep", "tp"), None)),
        check_vma=False,
    )
```
